512 devices in a mesh: sp: 32 (over z, core), tp: 16 (over y, x).
Axes of the slice: x: 4, y: 4, z: 16, core: 2. Of those that a mesh axis runs over, the one named last changes fastest.
Arguments:
- cotangent: bfloat16 [4096, 2048], P('sp'), may hold values from -6 to 6
- normed: bfloat16 [4096, 2048], P('sp'), may hold values from -6 to 6
- inverse_root_mean_square: float32 [4096], P('sp'), may hold values from 0.5 to 2
- expert_norm_scale: float32 [2048], replicated, may hold values from 0.1 to 1.9
- routes: int32 [4096, 2], P('sp'), may hold values from 0 to 31, all different within a row; in each aligned block of 128 rows (0 to 127, 128 to 255, ...) at most 16 rows name the same one
- route_probability_weight: float32 [4096, 2], P('sp'), may hold values from 0.2 to 1
- gate_weight: bfloat16 [32, 2048, 2048], P('sp', None, 'tp'), may hold values from -0.125 to 0.125
- up_weight: bfloat16 [32, 2048, 2048], P('sp', None, 'tp'), may hold values from -0.125 to 0.125
- down_weight: bfloat16 [32, 2048, 2048], P('sp', 'tp'), may hold values from -0.125 to 0.125
- recurrence_input: bfloat16 [4096, 1024], P('sp', 'tp'), may hold values from -6 to 6
- recurrence_gate_logits: bfloat16 [4096, 1024], P('sp', 'tp'), may hold values from -6 to 6
- input_gate_logits: bfloat16 [4096, 1024], P('sp', 'tp'), may hold values from -6 to 6
- channel_decay_weight: float32 [1024], P('tp'), may hold values from 3 to 20
- extra_log_decay: float32 [4096, 1024], P('sp', 'tp'), may hold values from -1 to 0
- output_matrix: bfloat16 [2048, 1024], P(None, 'tp'), may hold values from -0.1875 to 0.1875
Outputs:
- grad_gate: bfloat16 [32, 2048, 2048], P('sp', None, 'tp')
- grad_up: bfloat16 [32, 2048, 2048], P('sp', None, 'tp')
- grad_down: bfloat16 [32, 2048, 2048], P('sp', 'tp')
- grad_out_weight: float32 [2048, 1024], P('sp', 'tp')
- grad_rec_input: float32 [4096, 1024], P('sp', 'tp')
- grad_decay_gate: float32 [4096, 1024], P('sp', 'tp')
- grad_input_gate: float32 [4096, 1024], P('sp', 'tp')
The draws below stay inside these ranges and needn't reach their ends.
Inputs may be any that keep to these rules, and one draw needn't show every extreme that they name: `routes`: each row names 2 different experts; among the rows of one device no expert is named more than 16 times.
All inputs are finite; a program needn't handle non-finite values.
Results may differ from the reference program's by a relative error of at most 0.025.
Values may be sent and summed in bfloat16 or wider, within the bound.
A program may use at most 64 MiB of HBM per device.

```python
import math
import jax
import jax.numpy as jnp
import numpy as np
from jax import lax

D = 2048
C = 1024
FF = 2048
TOPK = 2
TOK_DEV = 128
EXPERTS = 32
CAP = 16
TOKENS = 4096
N_SP = 32
N_TP = 16


def draw_channel_decay_weight(key, part):
    first, second, third = jax.random.split(key, 3)
    share = 0.5
    quick = jax.random.uniform(first, (C,), jnp.float32) < share
    slow_rate = jnp.exp(jax.random.uniform(second, (C,), jnp.float32, jnp.log(0.02), jnp.log(0.12))) / TOKENS
    quick_rate = jnp.exp(jax.random.uniform(third, (C,), jnp.float32, jnp.log(0.005), jnp.log(0.02)))
    rate = jnp.where(quick, quick_rate, slow_rate)
    return (-jnp.log(jnp.expm1(rate))).astype(jnp.float32)


def draw_extra_log_decay(key, part):
    first, second = jax.random.split(key, 2)
    places = jax.random.randint(first, (3,), 0, TOKENS)
    struck = jnp.any(jnp.arange(TOKENS)[:, None] == places[None, :], axis=1)
    depth = jnp.log(jax.random.uniform(second, (TOKENS, C), jnp.float32, 0.65, 0.85))
    return jnp.where(struck[:, None], depth, 0.0).astype(jnp.float32)


def draw_recurrence_gate_logits(key, part):
    first, second = jax.random.split(key, 2)
    blocks = TOKENS // TOK_DEV
    offset = jax.random.uniform(first, (blocks,), jnp.float32, -1.0, 1.0)
    noise = jnp.clip(jax.random.normal(second, (TOKENS, C), jnp.float32) * 0.7, -3.5, 3.5)
    return (noise + jnp.repeat(offset, TOK_DEV)[:, None]).astype(jnp.bfloat16)


def raised(drawn, own_key, source, target, shards_of, factor):
    owner, partner = [(jnp.arange(drawn.shape[position]) // (drawn.shape[position] // shards_of)).reshape([-1 if axis == position else 1 for axis in range(drawn.ndim)]) for position in (source, target)]
    chosen = jax.random.permutation(own_key, shards_of)[partner]
    strong = (owner == chosen) | (owner == (partner + shards_of // 2) % shards_of)
    return jnp.where(strong, factor * drawn, drawn)


def shard_levels(stream_key, extent, cuts, least, largest):
    factor_of, own = 1.0, jax.random.fold_in(stream_key, 6)
    for axis_at, parts in cuts:
        draws = jnp.exp(jax.random.uniform(jax.random.fold_in(own, axis_at), (parts,), jnp.float32, least / len(cuts), largest / len(cuts)))
        factor_of = factor_of * jnp.repeat(draws, extent[axis_at] // parts).reshape([-1 if axis == axis_at else 1 for axis in range(len(extent))])
    return factor_of


def routed_block(key, own, number, rows, number_of, top, most, lean):
    order = jax.random.permutation(key, number_of)
    packed, ordinary = shares(number_of, rows * top, most, lean, True), shares(number_of, rows * top, most, lean, False)
    places = jnp.arange(number_of)

    def named(tallies, rotation):
        used = int((tallies > 0).sum())
        fixed = max(1, used // 4)
        moved = fixed + (places - fixed + rotation * (used - fixed)) % max(1, number_of - fixed)
        return jnp.zeros((number_of,), jnp.int32).at[order[jnp.where(places < fixed, places, moved)]].set(jnp.asarray(tallies, jnp.int32))

    tallies = jnp.where(number % 4 == 0, named(packed, number // 4), named(ordinary, number - number // 4 - 1))
    mixed = jax.random.permutation(jax.random.fold_in(own, 3), number_of)
    source_of, receiver = mixed[0:number_of // 2 * 2:2], mixed[1:number_of // 2 * 2:2]
    room = jnp.minimum(tallies[source_of] - 1, most - tallies[receiver]) // 2
    room = jnp.where((source_of == order[0]) | (receiver == order[0]) | (tallies[receiver] == 0), 0, jnp.maximum(room, 0))
    moved = jax.random.randint(jax.random.fold_in(own, 4), (number_of // 2,), 0, 1 << 20) % (room + 1)
    tallies = tallies.at[source_of].add(-moved).at[receiver].add(moved)
    items = jnp.searchsorted(jnp.cumsum(tallies), jnp.arange(rows * top), side="right").astype(jnp.int32)
    listing = items.reshape(top, rows).T
    listing = listing[jax.random.permutation(jax.random.fold_in(own, 1), rows)]
    rotation = jax.random.randint(jax.random.fold_in(own, 2), (rows, 1), 0, top)
    return jnp.take_along_axis(listing, (jnp.arange(top)[None, :] + rotation) % top, axis=1)


def shares(amount, total, most, lean, full):
    loads = [(1 << 20) // math.isqrt(grade ** lean) + 1 for grade in range(1, amount + 1)]
    largest = most if full else min(most, max(-(-total // amount), total * loads[0] // sum(loads)))
    least = 1 if total - largest >= amount - 1 else 0
    holding, rest = [largest] + [least] * (amount - 1), total - largest - least * (amount - 1)
    while rest > 0:
        candidates = [i for i in range(1, amount) if holding[i] < largest] or [i for i in range(1, amount) if holding[i] < most]
        pool, remaining = sum([loads[i] for i in candidates]), rest
        for i in candidates:
            addition = min(most - holding[i], max(1, remaining * loads[i] // pool), rest)
            holding[i] = holding[i] + addition
            rest = rest - addition
    return np.array(holding)


def gaussian(rng, shape, width, reach, cuts=(), kind=jnp.bfloat16):
    loudness = shard_levels(rng, shape, cuts, -0.22, 0.18) if cuts else 1.0
    values = jax.random.normal(rng, shape, jnp.float32) * width * loudness
    return jnp.minimum(jnp.maximum(values, -reach), reach).astype(kind)


def gaussian_with(own_key, extent, scale, bound, shards, heavy, kind=jnp.bfloat16):
    entries = scale * jax.random.normal(own_key, extent, jnp.float32)
    if shards:
        entries = entries * shard_levels(own_key, extent, shards, -0.22, 0.18)
    return jnp.clip(raised(entries, jax.random.fold_in(own_key, 3), *heavy), -bound, bound).astype(kind)


def setup_inputs(seed: int = 0) -> dict:
    key_list = jax.random.split(jax.random.key(seed), 16)
    cotangent = gaussian_with(key_list[0], (TOKENS, D), 1.0, 6.0, ((0, 32),), (0, 1, 32, 2.75))
    normed = gaussian(key_list[1], (TOKENS, D), 1.0, 6.0, ((0, 32),))
    inverse_root_mean_square = jnp.clip(jnp.exp(math.log(2.0) - 1.3862944 * jax.random.uniform(key_list[2], (TOKENS,), jnp.float32) ** shard_levels(key_list[2], (TOKENS,), ((0, 32),), -0.2, 0.2)), 0.5, 2.0)
    expert_norm_scale = jnp.clip(1.0 + 0.18 * jax.random.normal(key_list[3], (D,), jnp.float32), 0.1, 1.9)
    routes_keys = jax.random.split(jax.random.fold_in(key_list[4], 1), TOKENS // TOK_DEV)
    routes_turns = jax.random.permutation(jax.random.fold_in(key_list[4], 3), TOKENS // TOK_DEV)
    routes = jax.vmap(lambda own, number: routed_block(jax.random.fold_in(key_list[4], 2), own, number, TOK_DEV, EXPERTS, TOPK, CAP, 1))(routes_keys, routes_turns).reshape((TOKENS, TOPK))
    route_probability_weight = jnp.clip(0.2 + 0.8 * jax.random.uniform(key_list[5], (TOKENS, TOPK), jnp.float32) ** shard_levels(key_list[5], (TOKENS, TOPK), ((0, 32),), -0.2, 0.2), 0.2, 1.0)
    gate_weight = gaussian(key_list[6], (EXPERTS, D, FF), D ** -0.5, 0.125, ((0, 32), (2, 16)))
    up_weight = gaussian(key_list[7], (EXPERTS, D, FF), D ** -0.5, 0.125, ((0, 32), (2, 16)))
    down_weight = gaussian(key_list[8], (EXPERTS, FF, D), FF ** -0.5, 0.125, ((0, 32), (1, 16)))
    recurrence_input = gaussian(key_list[9], (TOKENS, C), 1.0, 6.0, ((0, 32), (1, 16)))
    recurrence_gate_logits = draw_recurrence_gate_logits(jax.random.fold_in(key_list[15], 71), 0)
    input_gate_logits = gaussian(key_list[11], (TOKENS, C), 1.0, 6.0, ((0, 32), (1, 16)))
    channel_decay_weight = draw_channel_decay_weight(jax.random.fold_in(key_list[15], 71), 0)
    extra_log_decay = draw_extra_log_decay(jax.random.fold_in(key_list[15], 71), 0)
    output_matrix = gaussian(key_list[14], (D, C), C ** -0.5, 0.1875, ((1, 16),))
    return dict(cotangent=cotangent, normed=normed, inverse_root_mean_square=inverse_root_mean_square, expert_norm_scale=expert_norm_scale, routes=routes, route_probability_weight=route_probability_weight, gate_weight=gate_weight, up_weight=up_weight, down_weight=down_weight, recurrence_input=recurrence_input, recurrence_gate_logits=recurrence_gate_logits, input_gate_logits=input_gate_logits, channel_decay_weight=channel_decay_weight, extra_log_decay=extra_log_decay, output_matrix=output_matrix)


def link(earlier, later):
    return (earlier[0] * later[0], later[0] * earlier[1] + later[1])

def expert_step(items):
    grad_in, tokens_in, gate_w, up_w, down_w = items
    rows = tokens_in.shape[0]
    gate_pre = jnp.dot(tokens_in, gate_w, preferred_element_type=jnp.float32)
    up_pre = jnp.dot(tokens_in, up_w, preferred_element_type=jnp.float32)
    sigma = jax.nn.sigmoid(gate_pre)
    swish = gate_pre * sigma
    active = (swish * up_pre).astype(jnp.bfloat16)
    d_active = jnp.dot(grad_in, down_w.T, preferred_element_type=jnp.float32)
    d_gate = (d_active * up_pre * sigma * (1.0 + gate_pre * (1.0 - sigma))).astype(jnp.bfloat16)
    d_up = (d_active * swish).astype(jnp.bfloat16)
    grad_down = jnp.dot(active.T, grad_in, preferred_element_type=jnp.float32).astype(jnp.bfloat16)
    grad_gate = jnp.dot(tokens_in.T, d_gate, preferred_element_type=jnp.float32).astype(jnp.bfloat16)
    grad_up = jnp.dot(tokens_in.T, d_up, preferred_element_type=jnp.float32).astype(jnp.bfloat16)
    block = FF // N_TP
    d_gate4 = d_gate.astype(jnp.float32).reshape(rows, N_TP, block)
    d_up4 = d_up.astype(jnp.float32).reshape(rows, N_TP, block)
    gate4 = gate_w.astype(jnp.float32).reshape(D, N_TP, block)
    up4 = up_w.astype(jnp.float32).reshape(D, N_TP, block)
    pieces = jnp.einsum('rjf,djf->jrd', d_gate4, gate4) + jnp.einsum('rjf,djf->jrd', d_up4, up4)
    rounded = lax.optimization_barrier(pieces.astype(jnp.bfloat16)).astype(jnp.float32)
    returned = lax.optimization_barrier(jnp.sum(rounded, axis=0)).astype(jnp.bfloat16)
    return (grad_gate, grad_up, grad_down, returned)

def reference(cotangent, normed, inverse_root_mean_square, expert_norm_scale, routes, route_probability_weight, gate_weight, up_weight, down_weight, recurrence_input, recurrence_gate_logits, input_gate_logits, channel_decay_weight, extra_log_decay, output_matrix):
    per_block = TOK_DEV * TOPK
    chosen = routes.reshape(N_SP, per_block)
    member = (chosen[:, :, None] == jnp.arange(EXPERTS, dtype=jnp.int32)[None, None, :]).astype(jnp.int32)
    ranking = lax.optimization_barrier(jnp.sum((jnp.cumsum(member, axis=1) - member) * member, axis=2))
    source = jnp.arange(N_SP, dtype=jnp.int32)[:, None]
    landing = (chosen * (N_SP * CAP) + source * CAP + ranking).reshape(-1).astype(jnp.int32)
    scaled = (route_probability_weight[:, :, None] * cotangent[:, None, :].astype(jnp.float32)).astype(jnp.bfloat16)
    scaled = scaled.reshape(TOKENS * TOPK, D)
    copies = jnp.repeat(normed, TOPK, axis=0)
    buffer_rows = EXPERTS * N_SP * CAP
    grad_in = jnp.zeros((buffer_rows, D), jnp.bfloat16).at[landing].set(scaled).reshape(EXPERTS, N_SP * CAP, D)
    tokens_in = jnp.zeros((buffer_rows, D), jnp.bfloat16).at[landing].set(copies).reshape(EXPERTS, N_SP * CAP, D)
    grad_gate, grad_up, grad_down, returned = lax.map(expert_step, (grad_in, tokens_in, gate_weight, up_weight, down_weight))
    back_rows = returned.reshape(buffer_rows, D)[landing]
    d_norm = lax.optimization_barrier(jnp.sum(back_rows.astype(jnp.float32).reshape(TOKENS, TOPK, D), axis=1))
    nhat = normed.astype(jnp.float32) / expert_norm_scale[None, :]
    gained = expert_norm_scale[None, :] * d_norm
    stat = lax.optimization_barrier(jnp.mean(gained * nhat, axis=1, keepdims=True))
    d_mix = (cotangent.astype(jnp.float32) + inverse_root_mean_square[:, None] * (gained - nhat * stat)).astype(jnp.bfloat16)
    retention_factor = jax.nn.sigmoid(recurrence_gate_logits.astype(jnp.float32))
    admit = jax.nn.sigmoid(input_gate_logits.astype(jnp.float32))
    signal = recurrence_input.astype(jnp.float32)
    decay_speed = jax.nn.softplus(-channel_decay_weight)
    log_retention = -8.0 * retention_factor * decay_speed[None, :] + extra_log_decay
    keep = jnp.exp(log_retention)
    scale_in = jnp.sqrt(-jnp.expm1(2.0 * log_retention))
    driven = scale_in * admit * signal
    _, state = lax.associative_scan(link, (keep, driven), axis=0)
    hidden = state.astype(jnp.bfloat16)
    state_prev = jnp.concatenate([jnp.zeros((1, C), jnp.float32), state[:-1]], axis=0)
    grad_out_weight = jnp.dot(d_mix.T, hidden, preferred_element_type=jnp.float32)
    d_state = jnp.dot(d_mix, output_matrix, preferred_element_type=jnp.float32)
    keep_next = jnp.concatenate([keep[1:], jnp.ones((1, C), jnp.float32)], axis=0)
    _, total = lax.associative_scan(link, (keep_next, d_state), reverse=True, axis=0)
    grad_rec_input = total * scale_in * admit
    grad_input_gate = total * scale_in * signal * admit * (1.0 - admit)
    d_log = total * state_prev * keep - total * admit * signal * keep * keep / scale_in
    grad_decay_gate = d_log * (-8.0 * decay_speed[None, :]) * retention_factor * (1.0 - retention_factor)
    return (grad_gate, grad_up, grad_down, grad_out_weight, grad_rec_input, grad_decay_gate, grad_input_gate)
```

```python
import functools

import jax
import jax.numpy as jnp
from jax import lax
from jax.experimental import pallas as pl
from jax.experimental.pallas import tpu as pltpu
from jax.sharding import PartitionSpec as P

MESH = pl.DeviceIdType.MESH
F32 = jnp.float32
BF16 = jnp.bfloat16
SIDE = 4
SHIFT = 3
COLS = 128
CAP = 16


def dot(a, b, ca, cb):
    return lax.dot_general(a, b, (((ca,), (cb,)), ((), ())), preferred_element_type=F32)


def take(ref, sem):
    pltpu.make_async_copy(ref, ref, sem).wait()


def send(src, dst, send_sem, recv_sem, target):
    pltpu.make_async_remote_copy(
        src_ref=src,
        dst_ref=dst,
        send_sem=send_sem,
        recv_sem=recv_sem,
        device_id=target,
        device_id_type=MESH,
    ).start()


class Gather:
    def __init__(self, block, i, axis_to, ss, rs):
        self.block, self.i, self.to, self.ss, self.rs = block, i, axis_to, ss, rs
        self.up, self.down, self.far = lax.rem(i + 1, 4), lax.rem(i + 3, 4), lax.rem(i + 2, 4)

    def go(self, src, half, target, k):
        ref = self.block(src, half)
        send(ref, ref, self.ss.at[k], self.rs.at[k], target)

    def first(self):
        self.go(self.i, None, self.to(self.up), 0)
        self.go(self.i, None, self.to(self.down), 1)

    def relay(self):
        take(self.block(self.down, None), self.rs.at[0])
        self.go(self.down, 0, self.to(self.up), 2)
        take(self.block(self.up, None), self.rs.at[1])
        self.go(self.up, 1, self.to(self.down), 3)

    def last(self):
        take(self.block(self.far, 0), self.rs.at[2])
        take(self.block(self.far, 1), self.rs.at[3])

    def sent(self):
        take(self.block(self.i, None), self.ss.at[0])
        take(self.block(self.i, None), self.ss.at[1])
        take(self.block(self.down, 0), self.ss.at[2])
        take(self.block(self.up, 1), self.ss.at[3])


class Scatter:
    def __init__(self, block, i, axis_to, ss, rs, part, low, high):
        self.block, self.i, self.to, self.ss, self.rs = block, i, axis_to, ss, rs
        self.part, self.low, self.high = part, low, high
        self.up, self.down, self.far = lax.rem(i + 1, 4), lax.rem(i + 3, 4), lax.rem(i + 2, 4)

    def go(self, src, dst, target, k):
        send(src, dst, self.ss.at[k], self.rs.at[k], target)

    def first(self):
        up, down = self.to(self.up), self.to(self.down)
        self.go(self.block(self.far, 0), self.part(0), up, 0)
        self.go(self.block(self.far, 1), self.part(1), down, 1)
        self.go(self.block(self.up, 1), self.low(1), up, 2)
        self.go(self.block(self.down, 0), self.high(0), down, 3)

    def relay(self):
        for k, (member, target, half, dst) in enumerate(
            ((self.up, self.up, 0, self.low(0)), (self.down, self.down, 1, self.high(1)))
        ):
            take(self.part(half), self.rs.at[k])
            ref = self.block(member, half)
            ref[...] = (ref[...].astype(F32) + self.part(half)[...].astype(F32)).astype(BF16)
            self.go(ref, dst, self.to(target), 4 + k)

    def last(self):
        take(self.low(1), self.rs.at[2])
        take(self.high(0), self.rs.at[3])
        take(self.low(0), self.rs.at[4])
        take(self.high(1), self.rs.at[5])

    def total(self, half):
        return (
            self.block(self.i, half)[...].astype(F32)
            + self.low(half)[...].astype(F32)
            + self.high(half)[...].astype(F32)
        )

    def sent(self):
        for k in range(6):
            take(self.part(0), self.ss.at[k])


def softplus(v):
    z = jnp.exp(-jnp.abs(v))
    s = z / (2.0 + z)
    q = s * s
    series = jnp.zeros_like(s)
    for k in range(9, -1, -1):
        series = series * q + 1.0 / (2 * k + 1)
    return jnp.maximum(v, 0.0) + 2.0 * s * series


def expm1(v):
    near = jnp.clip(v, -0.5, 0.5)
    series = jnp.ones_like(v)
    for k in range(10, 1, -1):
        series = 1.0 + near * series * (1.0 / k)
    return jnp.where(jnp.abs(v) < 0.5, near * series, jnp.exp(v) - 1.0)


def kernel(
    ns,
    cot,
    norm,
    irms,
    gain,
    routes,
    prob,
    gate_w,
    up_w,
    down_w,
    rec_in,
    rec_gate,
    in_gate,
    decay_w,
    extra,
    out_m,
    g_gate,
    g_up,
    g_down,
    g_out,
    g_rec,
    g_dec,
    g_in,
    packed,
    picked,
    rows,
    wide,
    d_wide,
    act,
    part,
    t_buf,
    lo_buf,
    hi_buf,
    s_buf,
    t2_buf,
    lo2_buf,
    hi2_buf,
    back,
    arrived,
    dn,
    d_mix,
    scan_a,
    scan_b,
    rows_f,
    lead,
    leads,
    trail,
    trails,
    coef,
    gw_all,
    gw_pair,
    gw_chip,
    gw_in,
    z_s,
    z_r,
    ag_s,
    ag_r,
    rs_s,
    rs_r,
    dn_s,
    dn_r,
    back_s,
    back_r,
    lead_s,
    lead_r,
    trail_s,
    trail_r,
    pair_s,
    pair_r,
    gw_s,
    gw_r,
):
    sp, tp = lax.axis_index("sp"), lax.axis_index("tp")
    z, core = lax.div(sp, 2), lax.rem(sp, 2)
    y, x = lax.div(tp, SIDE), lax.rem(tp, SIDE)
    nz = ns // 2
    tokens = norm.shape[0]
    near = nz // 2
    chunk = near * 2 * CAP

    def to_x(v):
        return {"sp": sp, "tp": y * SIDE + v}

    def to_y(v):
        return {"sp": sp, "tp": v * SIDE + x}

    def to_sp(v):
        return {"sp": v, "tp": tp}

    barrier = pltpu.get_barrier_semaphore()
    steps = [1, -1, 2, -2, 3, -3]
    steps = [d for d in steps] + [-4] + [4, 5, -5, 6, -6, 7, -7, 8]
    others = [(0, 1)] + [(d, c) for d in steps for c in (0, 1)]

    def other(d, c):
        if d == 0:
            return z * 2 + (1 - core)
        return lax.rem(z + d + nz, nz) * 2 + c

    for d, c in others:
        pl.semaphore_signal(barrier, inc=1, device_id=to_sp(other(d, c)), device_id_type=MESH)
    for v in (1, 3):
        pl.semaphore_signal(
            barrier, inc=1, device_id=to_x(lax.rem(x + v, SIDE)), device_id_type=MESH
        )
        pl.semaphore_signal(
            barrier, inc=1, device_id=to_y(lax.rem(y + v, SIDE)), device_id_type=MESH
        )

    mine = pl.ds(pl.multiple_of(tp * COLS, COLS), COLS)
    lane = lax.broadcasted_iota(jnp.int32, (tokens, ns), 1)
    chosen = [routes[:, k : k + 1] for k in (0, 1)]
    member = [(e == lane).astype(F32) for e in chosen]
    earlier = (
        lax.broadcasted_iota(jnp.int32, (tokens, tokens), 1)
        < lax.broadcasted_iota(jnp.int32, (tokens, tokens), 0)
    ).astype(BF16)
    before = dot(earlier, (member[0] + member[1]).astype(BF16), 1, 0)
    slot = lax.broadcasted_iota(jnp.int32, (tokens, ns * CAP), 1).astype(F32)
    at = [
        slot
        == (e.astype(F32) * CAP + jnp.sum(m * before, axis=1, keepdims=True))
        for e, m in zip(chosen, member)
    ]
    one = [a.astype(F32) for a in at]
    both = (one[0] + one[1]).astype(BF16)
    picked[...] = both
    own_cot = cot[:, mine].astype(F32)
    packed[0] = dot(both, norm[:, mine], 0, 0).astype(BF16)
    packed[1] = (
        dot(one[0].astype(BF16), (prob[:, 0:1] * own_cot).astype(BF16), 0, 0)
        + dot(one[1].astype(BF16), (prob[:, 1:2] * own_cot).astype(BF16), 0, 0)
    ).astype(BF16)

    pl.semaphore_wait(barrier, len(others) + 4)

    own_x = pl.ds(pl.multiple_of(x * COLS, COLS), COLS)

    def place(d):
        return lax.rem(SHIFT - d + 2 * nz, nz) if not isinstance(d, int) else (SHIFT - d) % nz

    def rows_at(pos, c):
        return pl.ds(pl.multiple_of((pos * 2 + c) * CAP, CAP), CAP)

    for d, c in others:
        target = other(d, c)
        k = 0 if place(d) < near else 1
        send(
            packed.at[:, pl.ds(pl.multiple_of(target * CAP, CAP), CAP), :],
            rows.at[:, y, rows_at(place(d), core), own_x],
            z_s.at[k],
            z_r.at[k],
            to_sp(target),
        )
    pltpu.make_async_copy(
        packed.at[:, pl.ds(pl.multiple_of(sp * CAP, CAP), CAP), :],
        rows.at[:, y, rows_at(SHIFT, core), own_x],
        z_r.at[0],
    ).start()

    channels = extra.shape[1]
    retain = jax.nn.sigmoid(rec_gate[...].astype(F32))
    admit = jax.nn.sigmoid(in_gate[...].astype(F32))
    signal = rec_in[...].astype(F32)
    speed = -8.0 * softplus(-decay_w[...])
    log_keep = retain * speed + extra[...]
    keep = jnp.exp(log_keep)
    scale_in = jnp.sqrt(-expm1(2.0 * log_keep))
    pad = 64
    scan_a[pl.ds(0, pad), :] = jnp.ones((pad, channels), F32)
    scan_a[pl.ds(pad + tokens, pad), :] = jnp.ones((pad, channels), F32)
    scan_b[pl.ds(0, pad), :] = jnp.zeros((pad, channels), F32)
    scan_b[pl.ds(pad + tokens, pad), :] = jnp.zeros((pad, channels), F32)
    body = pl.ds(pad, tokens)

    def scan(a, b, sign):
        step = 1
        while step < tokens:
            scan_a[body, :] = a
            scan_b[body, :] = b
            moved = pl.ds(pad - sign * step, tokens)
            b = a * scan_b[moved, :] + b
            a = a * scan_a[moved, :]
            step *= 2
        return a, b

    keep_cum, state_loc = scan(keep, scale_in * admit * signal, 1)
    lead[...] = jnp.concatenate(
        [keep_cum[tokens - 1 :, :], state_loc[tokens - 1 :, :]], axis=1
    )
    leads[sp] = lead[...]
    for d, c in others:
        send(lead, leads.at[sp], lead_s, lead_r, to_sp(other(d, c)))
    scan_a[body, :] = keep
    keep_next = scan_a[pl.ds(pad + 1, tokens), :]
    rows_f[0] = keep_cum
    rows_f[1] = state_loc
    rows_f[2] = keep
    rows_f[3] = keep_next
    rows_f[4] = scale_in * admit
    rows_f[5] = scale_in * signal * admit * (1.0 - admit)
    rows_f[6] = admit * signal * keep * keep / scale_in
    rows_f[7] = speed * retain * (1.0 - retain)
    wide[:, :COLS] = gate_w[0]
    wide[:, COLS:] = up_w[0]

    def z_arrived(k):
        take(rows.at[:, y, pl.ds(k * chunk, chunk), own_x], z_r.at[k])

    def gathers(k):
        base, half_rows = k * chunk, chunk // 2

        def span(half):
            if half is None:
                return pl.ds(base, chunk)
            return pl.ds(base + half * half_rows, half_rows)

        def at_x(i):
            return pl.ds(pl.multiple_of(i * COLS, COLS), COLS)

        blocks = (
            (lambda i, h: rows.at[0, y, span(h), at_x(i)], x, to_x),
            (lambda i, h: rows.at[1, i, span(h), own_x], y, to_y),
            (lambda i, h: rows.at[0, i, span(h), :], y, to_y),
            (lambda i, h: rows.at[1, :, span(h), at_x(i)], x, to_x),
        )
        made = [
            Gather(b, i, to, ag_s.at[4 * k + n], ag_r.at[4 * k + n])
            for n, (b, i, to) in enumerate(blocks)
        ]
        return made[:2], made[2:]

    def expert(k):
        span = pl.ds(k * chunk, chunk)
        deep = rows.shape[3]
        hidden = jnp.zeros((chunk, 2 * COLS), F32)
        d_act = jnp.zeros((chunk, COLS), F32)
        for j in range(SIDE):
            hidden += dot(rows[0, j, span, :], wide[j * deep : (j + 1) * deep, :], 1, 0)
            d_act += dot(rows[1, j, span, :], down_w[0, :, j * deep : (j + 1) * deep], 1, 1)
        gate_pre, up_pre = hidden[:, :COLS], hidden[:, COLS:]
        sigma = jax.nn.sigmoid(gate_pre)
        swish = gate_pre * sigma
        act[span, :] = (swish * up_pre).astype(BF16)
        d_wide[span, :COLS] = (
            d_act * up_pre * sigma * (1.0 + gate_pre * (1.0 - sigma))
        ).astype(BF16)
        d_wide[span, COLS:] = (d_act * swish).astype(BF16)
        for j in range(SIDE):
            for i in range(0, SIDE, 2):
                low = (j * SIDE + i) * COLS
                piece = dot(d_wide[span, :], wide[low : low + 2 * COLS, :], 1, 1).astype(BF16)
                part[j, i, span, :] = piece[:, :COLS]
                part[j, i + 1, span, :] = piece[:, COLS:]

    def scatters(k):
        base, half, quarter = k * chunk, chunk // 2, chunk // 4

        def span(start, h):
            return pl.ds(start + h * quarter, quarter)

        def full(buf, n):
            return lambda h: buf.at[n, :, pl.ds(h * quarter, quarter), :]

        def flat(buf, n):
            return lambda h: buf.at[n, pl.ds(h * quarter, quarter), :]

        n = 2 * k
        made = (
            Scatter(
                lambda i, h: part.at[:, i, span(base, h), :], x, to_x,
                rs_s.at[4 * k], rs_r.at[4 * k],
                lambda h: t_buf.at[n, h], full(lo_buf, n), full(hi_buf, n),
            ),
            Scatter(
                lambda i, h: part.at[i, :, span(base + half, h), :], y, to_y,
                rs_s.at[4 * k + 1], rs_r.at[4 * k + 1],
                lambda h: t_buf.at[n + 1, h], full(lo_buf, n + 1), full(hi_buf, n + 1),
            ),
            Scatter(
                lambda i, h: s_buf.at[n, i, pl.ds(h * quarter, quarter), :], y, to_y,
                rs_s.at[4 * k + 2], rs_r.at[4 * k + 2],
                lambda h: t2_buf.at[n, h], flat(lo2_buf, n), flat(hi2_buf, n),
            ),
            Scatter(
                lambda i, h: s_buf.at[n + 1, i, pl.ds(h * quarter, quarter), :], x, to_x,
                rs_s.at[4 * k + 3], rs_r.at[4 * k + 3],
                lambda h: t2_buf.at[n + 1, h], flat(lo2_buf, n + 1), flat(hi2_buf, n + 1),
            ),
        )
        return made[:2], made[2:]

    def between(k, first):
        quarter = chunk // 4
        for n, ring in enumerate(first):
            for h in (0, 1):
                s_buf[2 * k + n, :, pl.ds(h * quarter, quarter), :] = ring.total(h).astype(BF16)

    def give_back(k, second):
        half, quarter = chunk // 2, chunk // 4
        for n, ring in enumerate(second):
            for h in (0, 1):
                back[pl.ds(k * chunk + n * half + h * quarter, quarter), :] = ring.total(h).astype(
                    BF16
                )
        dst = arrived.at[pl.ds(pl.multiple_of(sp * CAP, CAP), CAP), :]
        for d, c in others:
            pos = place(-d)
            if (pos < near) != (k == 0):
                continue
            where = rows_at(pos, 1 - core if d == 0 else c)
            send(back.at[where, :], dst, back_s.at[k], back_r, to_sp(other(d, c)))
        if k == 0:
            pltpu.make_async_copy(back.at[rows_at(SHIFT, core), :], dst, back_r).start()

    def each(rings, name):
        for ring in rings:
            getattr(ring, name)()

    a0, b0 = gathers(0)
    a1, b1 = gathers(1)
    r0, q0 = scatters(0)
    r1, q1 = scatters(1)

    z_arrived(0)
    each(a0, "first")
    each(a0, "relay")
    each(a0, "last")
    each(b0, "first")
    z_arrived(1)
    each(a1, "first")
    each(b0, "relay")
    each(a1, "relay")
    each(b0, "last")
    each(a1, "last")
    each(b1, "first")
    expert(0)
    each(r0, "first")
    each(b1, "relay")
    each(r0, "relay")
    each(r0, "last")
    between(0, r0)
    each(q0, "first")
    each(b1, "last")
    expert(1)
    each(r1, "first")
    each(q0, "relay")
    each(q0, "last")
    give_back(0, q0)
    each(r1, "relay")
    each(r1, "last")
    between(1, r1)
    each(q1, "first")
    each(q1, "relay")
    each(q1, "last")
    give_back(1, q1)

    deep = rows.shape[3]
    for j in range(SIDE):
        grads = dot(rows[0, j], d_wide[...], 0, 0).astype(BF16)
        g_gate[0, j * deep : (j + 1) * deep, :] = grads[:, :COLS]
        g_up[0, j * deep : (j + 1) * deep, :] = grads[:, COLS:]
        g_down[0, :, j * deep : (j + 1) * deep] = dot(act[...], rows[1, j], 0, 0).astype(BF16)

    take(leads.at[pl.ds(0, ns - 1)], lead_r)
    state_in = jnp.zeros((1, channels), F32)
    for i in range(ns):
        v = leads[i]
        state_in = jnp.where(i < sp, v[:, :channels] * state_in + v[:, channels:], state_in)
    run = jnp.ones((1, channels), F32)
    for i in range(ns):
        coef[i] = jnp.where(i > sp, run, 0.0)
        run = jnp.where(i > sp, run * leads[i][:, :channels], run)
    state = rows_f[1] + rows_f[0] * state_in
    scan_b[body, :] = state
    first_row = lax.broadcasted_iota(jnp.int32, (tokens, channels), 0) == 0
    state_prev = jnp.where(first_row, state_in, scan_b[pl.ds(pad - 1, tokens), :])
    rows_f[6] = (state_prev * rows_f[2] - rows_f[6]) * rows_f[7]
    hidden = state.astype(BF16)

    take(arrived, back_r)
    dn[y, :, own_x] = dot(picked[...], arrived[...], 1, 0).astype(BF16)
    half = tokens // 2
    quarter = tokens // 4

    def at_x(i):
        return pl.ds(pl.multiple_of(i * COLS, COLS), COLS)

    def piece(start, h):
        return pl.ds(start, half) if h is None else pl.ds(start + h * quarter, quarter)

    shapes = (
        (lambda i, h: dn.at[y, piece(0, h), at_x(i)], x, to_x),
        (lambda i, h: dn.at[i, piece(half, h), own_x], y, to_y),
        (lambda i, h: dn.at[i, piece(0, h), :], y, to_y),
        (lambda i, h: dn.at[:, piece(half, h), at_x(i)], x, to_x),
    )
    dg = [Gather(b, i, to, dn_s.at[n], dn_r.at[n]) for n, (b, i, to) in enumerate(shapes)]
    for pair in (dg[:2], dg[2:]):
        each(pair, "first")
        each(pair, "relay")
        each(pair, "last")

    eye = lax.broadcasted_iota(jnp.int32, (tokens, tokens), 0) == lax.broadcasted_iota(
        jnp.int32, (tokens, tokens), 1
    )
    inv_rms = jnp.sum(jnp.where(eye, irms[...], 0.0), axis=1, keepdims=True)
    stat = jnp.zeros((tokens, 1), F32)
    for j in range(SIDE):
        cols = pl.ds(j * deep, deep)
        g = gain[:, cols]
        stat += jnp.sum(
            (g * dn[j].astype(F32)) * (norm[:, cols].astype(F32) / g), axis=1, keepdims=True
        )
    stat = stat / norm.shape[1]
    for j in range(SIDE):
        cols = pl.ds(j * deep, deep)
        g = gain[:, cols]
        mix = cot[:, cols].astype(F32) + inv_rms * (
            g * dn[j].astype(F32) - (norm[:, cols].astype(F32) / g) * stat
        )
        d_mix[:, cols] = mix.astype(BF16)

    d_state = dot(d_mix[...], out_m[...], 1, 0)
    tail, grad_loc = scan(rows_f[3], d_state, -1)
    first_grad = rows_f[2][:1, :] * grad_loc[:1, :]
    trail[...] = jnp.concatenate([first_grad, first_grad], axis=1)
    trails[sp] = trail[...]
    for d, c in others:
        send(trail, trails.at[sp], trail_s, trail_r, to_sp(other(d, c)))

    g_rows = g_out.shape[0]
    gw = dot(d_mix[...], hidden, 0, 0).astype(BF16)
    for n in range(ns):
        low = n * g_rows
        gw_all[n % 2, n // 2] = jnp.concatenate(
            [gw[low : low + g_rows // 2, :], gw[low + g_rows // 2 : low + g_rows, :]], axis=1
        )
    send(gw_all.at[1 - core], gw_pair, pair_s, pair_r, to_sp(z * 2 + 1 - core))
    take(trails.at[pl.ds(0, ns - 1)], trail_r)
    entering = jnp.zeros((1, channels), F32)
    for i in range(ns):
        entering += coef[i] * trails[i][:, :channels]
    total = grad_loc + tail * entering
    take(gw_pair, pair_r)
    gw_chip[...] = (gw_all[core].astype(F32) + gw_pair[...].astype(F32)).astype(BF16)
    for d in steps:
        zz = lax.rem(z + d + nz, nz)
        send(gw_chip.at[zz], gw_in.at[z], gw_s, gw_r, to_sp(zz * 2 + core))
    pltpu.make_async_copy(gw_chip.at[z], gw_in.at[z], gw_r).start()
    g_rec[...] = total * rows_f[4]
    g_in[...] = total * rows_f[5]
    g_dec[...] = total * rows_f[6]
    take(gw_in, gw_r)
    acc = jnp.zeros((g_rows // 2, 2 * channels), F32)
    for i in range(nz):
        acc += gw_in[i].astype(F32)
    g_out[: g_rows // 2, :] = acc[:, :channels]
    g_out[g_rows // 2 :, :] = acc[:, channels:]

    block = ns // 2 * CAP
    take(packed.at[:, pl.ds(0, block - CAP), :], z_s.at[0])
    take(packed.at[:, pl.ds(0, block), :], z_s.at[1])
    for ring in a0 + b0 + a1 + b1 + list(r0) + list(q0) + list(r1) + list(q1) + dg:
        ring.sent()
    take(back.at[pl.ds(0, block - CAP), :], back_s.at[0])
    take(back.at[pl.ds(0, block), :], back_s.at[1])
    take(leads.at[pl.ds(0, ns - 1)], lead_s)
    take(trails.at[pl.ds(0, ns - 1)], trail_s)
    take(gw_pair, pair_s)
    take(gw_in.at[pl.ds(0, nz - 1)], gw_s)


def shards(
    cotangent,
    normed,
    inverse_root_mean_square,
    expert_norm_scale,
    routes,
    route_probability_weight,
    gate_weight,
    up_weight,
    down_weight,
    recurrence_input,
    recurrence_gate_logits,
    input_gate_logits,
    channel_decay_weight,
    extra_log_decay,
    output_matrix,
):
    ns = lax.axis_size("sp")
    tokens, features = normed.shape
    channels = recurrence_input.shape[1]
    slots = ns * CAP
    chunk, quarter = slots // 2, slots // 8
    wide = features // SIDE
    vmem, dma = pltpu.VMEM, pltpu.SemaphoreType.DMA
    args = (
        cotangent,
        normed,
        inverse_root_mean_square.reshape(1, tokens),
        expert_norm_scale.reshape(1, features),
        routes,
        route_probability_weight,
        gate_weight,
        up_weight,
        down_weight,
        recurrence_input,
        recurrence_gate_logits,
        input_gate_logits,
        channel_decay_weight.reshape(1, channels),
        extra_log_decay,
        output_matrix,
    )
    f32_rows = jax.ShapeDtypeStruct((tokens, channels), F32)
    return pl.pallas_call(
        functools.partial(kernel, ns),
        out_shape=(
            jax.ShapeDtypeStruct(gate_weight.shape, BF16),
            jax.ShapeDtypeStruct(up_weight.shape, BF16),
            jax.ShapeDtypeStruct(down_weight.shape, BF16),
            jax.ShapeDtypeStruct((features // ns, channels), F32),
            f32_rows,
            f32_rows,
            f32_rows,
        ),
        in_specs=[pl.BlockSpec(memory_space=pltpu.VMEM)] * len(args),
        out_specs=[pl.BlockSpec(memory_space=pltpu.VMEM)] * 7,
        scratch_shapes=[
            vmem((2, slots, COLS), BF16),
            vmem((tokens, slots), BF16),
            vmem((2, SIDE, slots, wide), BF16),
            vmem((features, 2 * COLS), BF16),
            vmem((slots, 2 * COLS), BF16),
            vmem((slots, COLS), BF16),
            vmem((SIDE, SIDE, slots, COLS), BF16),
            vmem((4, 2, SIDE, quarter, COLS), BF16),
            vmem((4, SIDE, 2 * quarter, COLS), BF16),
            vmem((4, SIDE, 2 * quarter, COLS), BF16),
            vmem((4, SIDE, 2 * quarter, COLS), BF16),
            vmem((4, 2, quarter, COLS), BF16),
            vmem((4, 2 * quarter, COLS), BF16),
            vmem((4, 2 * quarter, COLS), BF16),
            vmem((slots, COLS), BF16),
            vmem((slots, COLS), BF16),
            vmem((SIDE, tokens, wide), BF16),
            vmem((tokens, features), BF16),
            vmem((tokens + 128, channels), F32),
            vmem((tokens + 128, channels), F32),
            vmem((8, tokens, channels), F32),
            vmem((1, 2 * channels), F32),
            vmem((ns, 1, 2 * channels), F32),
            vmem((1, 2 * channels), F32),
            vmem((ns, 1, 2 * channels), F32),
            vmem((ns, 1, channels), F32),
            vmem((2, ns // 2, features // ns // 2, 2 * channels), BF16),
            vmem((ns // 2, features // ns // 2, 2 * channels), BF16),
            vmem((ns // 2, features // ns // 2, 2 * channels), BF16),
            vmem((ns // 2, features // ns // 2, 2 * channels), BF16),
            dma((2,)),
            dma((2,)),
            dma((8, 4)),
            dma((8, 4)),
            dma((8, 6)),
            dma((8, 6)),
            dma((4, 4)),
            dma((4, 4)),
            dma((2,)),
            dma,
            dma,
            dma,
            dma,
            dma,
            dma,
            dma,
            dma,
            dma,
        ],
        compiler_params=pltpu.CompilerParams(
            collective_id=0, has_side_effects=True, vmem_limit_bytes=60 * 1024 * 1024
        ),
    )(*args)


def solution(mesh):
    placed = (
        P("sp", None),
        P("sp", None),
        P("sp"),
        P(),
        P("sp", None),
        P("sp", None),
        P("sp", None, "tp"),
        P("sp", None, "tp"),
        P("sp", "tp", None),
        P("sp", "tp"),
        P("sp", "tp"),
        P("sp", "tp"),
        P("tp"),
        P("sp", "tp"),
        P(None, "tp"),
    )
    return jax.shard_map(
        shards,
        mesh=mesh,
        in_specs=placed,
        out_specs=(
            P("sp", None, "tp"),
            P("sp", None, "tp"),
            P("sp", "tp", None),
            P("sp", "tp"),
            P("sp", "tp"),
            P("sp", "tp"),
            P("sp", "tp"),
        ),
        check_vma=False,
    )
```

```python
import functools

import jax
import jax.numpy as jnp
from jax import lax
from jax.experimental import pallas as pl
from jax.experimental.pallas import tpu as pltpu
from jax.sharding import PartitionSpec as P

MESH = pl.DeviceIdType.MESH
F32 = jnp.float32
BF16 = jnp.bfloat16
SIDE = 4
SHIFT = 3
COLS = 128
CAP = 16
FULL = 67_043_328


def dot(a, b, ca, cb):
    return lax.dot_general(a, b, (((ca,), (cb,)), ((), ())), preferred_element_type=F32)


def take(ref, sem):
    pltpu.make_async_copy(ref, ref, sem).wait()


def send(src, dst, send_sem, recv_sem, target):
    pltpu.make_async_remote_copy(
        src_ref=src,
        dst_ref=dst,
        send_sem=send_sem,
        recv_sem=recv_sem,
        device_id=target,
        device_id_type=MESH,
    ).start()


class Gather:
    def __init__(self, block, i, axis_to, ss, rs):
        self.block, self.i, self.to, self.ss, self.rs = block, i, axis_to, ss, rs
        self.up, self.down, self.far = lax.rem(i + 1, 4), lax.rem(i + 3, 4), lax.rem(i + 2, 4)

    def go(self, src, half, target, k):
        ref = self.block(src, half)
        send(ref, ref, self.ss.at[k], self.rs.at[k], target)

    def first(self):
        self.go(self.i, None, self.to(self.up), 0)
        self.go(self.i, None, self.to(self.down), 1)

    def relay(self):
        take(self.block(self.down, None), self.rs.at[0])
        self.go(self.down, 0, self.to(self.up), 2)
        take(self.block(self.up, None), self.rs.at[1])
        self.go(self.up, 1, self.to(self.down), 3)

    def last(self):
        take(self.block(self.far, 0), self.rs.at[2])
        take(self.block(self.far, 1), self.rs.at[3])

    def sent(self):
        take(self.block(self.i, None), self.ss.at[0])
        take(self.block(self.i, None), self.ss.at[1])
        take(self.block(self.down, 0), self.ss.at[2])
        take(self.block(self.up, 1), self.ss.at[3])


class Scatter:
    def __init__(self, block, i, axis_to, ss, rs, part, low, high):
        self.block, self.i, self.to, self.ss, self.rs = block, i, axis_to, ss, rs
        self.part, self.low, self.high = part, low, high
        self.up, self.down, self.far = lax.rem(i + 1, 4), lax.rem(i + 3, 4), lax.rem(i + 2, 4)

    def go(self, src, dst, target, k):
        send(src, dst, self.ss.at[k], self.rs.at[k], target)

    def first(self):
        up, down = self.to(self.up), self.to(self.down)
        self.go(self.block(self.far, 0), self.part(0), up, 0)
        self.go(self.block(self.far, 1), self.part(1), down, 1)
        self.go(self.block(self.up, 1), self.low(1), up, 2)
        self.go(self.block(self.down, 0), self.high(0), down, 3)

    def relay(self):
        for k, (member, target, half, dst) in enumerate(
            ((self.up, self.up, 0, self.low(0)), (self.down, self.down, 1, self.high(1)))
        ):
            take(self.part(half), self.rs.at[k])
            ref = self.block(member, half)
            ref[...] = (ref[...].astype(F32) + self.part(half)[...].astype(F32)).astype(BF16)
            self.go(ref, dst, self.to(target), 4 + k)

    def last(self):
        take(self.low(1), self.rs.at[2])
        take(self.high(0), self.rs.at[3])
        take(self.low(0), self.rs.at[4])
        take(self.high(1), self.rs.at[5])

    def total(self, half):
        return (
            self.block(self.i, half)[...].astype(F32)
            + self.low(half)[...].astype(F32)
            + self.high(half)[...].astype(F32)
        )

    def sent(self):
        for k in range(6):
            take(self.part(0), self.ss.at[k])


def softplus(v):
    z = jnp.exp(-jnp.abs(v))
    s = z / (2.0 + z)
    q = s * s
    series = jnp.zeros_like(s)
    for k in range(9, -1, -1):
        series = series * q + 1.0 / (2 * k + 1)
    return jnp.maximum(v, 0.0) + 2.0 * s * series


def expm1(v):
    near = jnp.clip(v, -0.5, 0.5)
    series = jnp.ones_like(v)
    for k in range(10, 1, -1):
        series = 1.0 + near * series * (1.0 / k)
    return jnp.where(jnp.abs(v) < 0.5, near * series, jnp.exp(v) - 1.0)


def kernel(
    ns,
    cot_h,
    norm_h,
    irms_h,
    gain_h,
    routes_h,
    prob_h,
    gate_h,
    up_h,
    down_h,
    rec_in_h,
    rec_gate_h,
    in_gate_h,
    decay_h,
    extra_h,
    out_h,
    g_gate_h,
    g_up_h,
    g_down_h,
    g_out,
    g_rec,
    g_dec,
    g_in,
    packed,
    picked,
    rows,
    wide,
    d_wide,
    act,
    part,
    t_buf,
    lo_buf,
    hi_buf,
    s_buf,
    t2_buf,
    lo2_buf,
    hi2_buf,
    back,
    arrived,
    dn,
    d_mix,
    rows_f,
    lead,
    leads,
    trail,
    trails,
    coef,
    gw_all,
    gw_pair,
    gw_chip,
    gw_in,
    down_w,
    g_gate,
    g_up,
    g_down,
    cot,
    norm,
    irms,
    gain,
    routes,
    prob,
    rec_in,
    rec_gate,
    in_gate,
    decay_w,
    extra,
    out_m,
    w_r,
    g_s,
    z_s,
    z_r,
    ag_s,
    ag_r,
    rs_s,
    rs_r,
    dn_s,
    dn_r,
    back_s,
    back_r,
    lead_s,
    lead_r,
    trail_s,
    trail_r,
    pair_s,
    pair_r,
    gw_s,
    gw_r,
):
    sp, tp = lax.axis_index("sp"), lax.axis_index("tp")
    z, core = lax.div(sp, 2), lax.rem(sp, 2)
    y, x = lax.div(tp, SIDE), lax.rem(tp, SIDE)
    nz = ns // 2
    tokens = norm.shape[0]
    near = nz // 2
    chunk = near * 2 * CAP

    def to_x(v):
        return {"sp": sp, "tp": y * SIDE + v}

    def to_y(v):
        return {"sp": sp, "tp": v * SIDE + x}

    def to_sp(v):
        return {"sp": v, "tp": tp}

    barrier = pltpu.get_barrier_semaphore()
    steps = [1, -1, 2, -2, 3, -3]
    steps = [d for d in steps] + [-4] + [4, 5, -5, 6, -6, 7, -7, 8]
    others = [(0, 1)] + [(d, c) for d in steps for c in (0, 1)]

    def far_first(pairs):
        near_ones = [p for p in pairs if place(p[0]) < near]
        return near_ones[::-1] + [p for p in pairs if place(p[0]) >= near][::-1]

    def place(d):
        return (SHIFT - d) % nz

    def other(d, c):
        if d == 0:
            return z * 2 + (1 - core)
        return lax.rem(z + d + nz, nz) * 2 + c

    for d, c in others:
        pl.semaphore_signal(barrier, inc=1, device_id=to_sp(other(d, c)), device_id_type=MESH)
    for v in (1, 3):
        pl.semaphore_signal(
            barrier, inc=1, device_id=to_x(lax.rem(x + v, SIDE)), device_id_type=MESH
        )
        pl.semaphore_signal(
            barrier, inc=1, device_id=to_y(lax.rem(y + v, SIDE)), device_id_type=MESH
        )

    moves = (
        (routes_h, routes),
        (prob_h, prob),
        (norm_h, norm),
        (cot_h, cot),
        (rec_gate_h, rec_gate),
        (in_gate_h, in_gate),
        (rec_in_h, rec_in),
        (decay_h, decay_w),
        (extra_h, extra),
        (gate_h.at[0], wide.at[:, :COLS]),
        (up_h.at[0], wide.at[:, COLS:]),
        (down_h.at[0], down_w),
        (irms_h, irms),
        (gain_h, gain),
        (out_h, out_m),
    )
    moves = [pltpu.make_async_copy(a, b, w_r.at[k]) for k, (a, b) in enumerate(moves)]
    for copy in moves:
        copy.start()

    def have(first, last):
        for copy in moves[first:last]:
            copy.wait()

    mine = pl.ds(pl.multiple_of(tp * COLS, COLS), COLS)
    def eye(n):
        return lax.broadcasted_iota(jnp.int32, (n, n), 0) == lax.broadcasted_iota(
            jnp.int32, (n, n), 1
        )

    square = eye(tokens)

    def upright(row):
        return jnp.sum(jnp.where(square, row, 0.0), axis=1, keepdims=True)

    have(0, 4)
    expert_id = lax.broadcasted_iota(jnp.int32, (ns, tokens), 0)
    chosen = [routes[k : k + 1, :] for k in (0, 1)]
    member = [(e == expert_id).astype(F32) for e in chosen]
    earlier = (
        lax.broadcasted_iota(jnp.int32, (tokens, tokens), 0)
        < lax.broadcasted_iota(jnp.int32, (tokens, tokens), 1)
    ).astype(BF16)
    before = dot((member[0] + member[1]).astype(BF16), earlier, 1, 0)
    slot = lax.broadcasted_iota(jnp.int32, (ns * CAP, tokens), 0).astype(F32)
    one = [
        (slot == (e.astype(F32) * CAP + jnp.sum(m * before, axis=0, keepdims=True))).astype(F32)
        for e, m in zip(chosen, member)
    ]
    both = (one[0] + one[1]).astype(BF16)
    picked[...] = both
    own_cot = cot[:, mine].astype(F32)
    packed[0] = dot(both, norm[:, mine], 1, 0).astype(BF16)
    packed[1] = (
        dot(one[0].astype(BF16), (upright(prob[0:1, :]) * own_cot).astype(BF16), 1, 0)
        + dot(one[1].astype(BF16), (upright(prob[1:2, :]) * own_cot).astype(BF16), 1, 0)
    ).astype(BF16)

    with jax.named_scope("barrier"):
        pl.semaphore_wait(barrier, len(others) + 4)

    own_x = pl.ds(pl.multiple_of(x * COLS, COLS), COLS)

    def rows_at(pos, c):
        return pl.ds(pl.multiple_of((pos * 2 + c) * CAP, CAP), CAP)

    for d, c in far_first(others):
        target = other(d, c)
        k = 0 if place(d) < near else 1
        send(
            packed.at[:, pl.ds(pl.multiple_of(target * CAP, CAP), CAP), :],
            rows.at[:, y, rows_at(place(d), core), own_x],
            z_s.at[k],
            z_r.at[k],
            to_sp(target),
        )
    pltpu.make_async_copy(
        packed.at[:, pl.ds(pl.multiple_of(sp * CAP, CAP), CAP), :],
        rows.at[:, y, rows_at(SHIFT, core), own_x],
        z_r.at[0],
    ).start()

    channels = extra.shape[0]
    corner = eye(channels)

    def lying(column):
        return jnp.sum(jnp.where(corner, column, 0.0), axis=0, keepdims=True)

    def standing(row):
        return jnp.sum(jnp.where(corner, row, 0.0), axis=1, keepdims=True)

    token = lax.broadcasted_iota(jnp.int32, (channels, tokens), 1)

    def moved(v, step, fill):
        inside = token >= step if step > 0 else token < tokens + step
        return jnp.where(inside, pltpu.roll(v, step % tokens, 1), fill)

    def scan(a, b, sign):
        step = 1
        while step < tokens:
            b = a * moved(b, sign * step, 0.0) + b
            a = a * moved(a, sign * step, 1.0)
            step *= 2
        return a, b

    with jax.named_scope("recur"):
        have(4, 9)
        retain = jax.nn.sigmoid(rec_gate[...].astype(F32))
        admit = jax.nn.sigmoid(in_gate[...].astype(F32))
        signal = rec_in[...].astype(F32)
        speed = standing(-8.0 * softplus(-decay_w[...]))
        log_keep = retain * speed + extra[...]
        keep = jnp.exp(log_keep)
        scale_in = jnp.sqrt(-expm1(2.0 * log_keep))
        keep_cum, state_loc = scan(keep, scale_in * admit * signal, 1)
        lead[...] = jnp.concatenate(
            [lying(keep_cum[:, tokens - 1 :]), lying(state_loc[:, tokens - 1 :])], axis=1
        )
        leads[sp] = lead[...]
        for d, c in others:
            send(lead, leads.at[sp], lead_s, lead_r, to_sp(other(d, c)))
        rows_f[0] = keep_cum
        rows_f[1] = state_loc
        rows_f[2] = keep
        rows_f[3] = moved(keep, -1, 1.0)
        rows_f[4] = scale_in * admit
        rows_f[5] = scale_in * signal * admit * (1.0 - admit)
        rows_f[6] = admit * signal * keep * keep / scale_in
        rows_f[7] = speed * retain * (1.0 - retain)

    def z_arrived(k):
        with jax.named_scope(f"z_arrived{k}"):
            take(rows.at[:, y, pl.ds(k * chunk, chunk), own_x], z_r.at[k])

    def gathers(k):
        base, half_rows = k * chunk, chunk // 2

        def span(half):
            if half is None:
                return pl.ds(base, chunk)
            return pl.ds(base + half * half_rows, half_rows)

        def at_x(i):
            return pl.ds(pl.multiple_of(i * COLS, COLS), COLS)

        blocks = (
            (lambda i, h: rows.at[0, y, span(h), at_x(i)], x, to_x),
            (lambda i, h: rows.at[1, i, span(h), own_x], y, to_y),
            (lambda i, h: rows.at[0, i, span(h), :], y, to_y),
            (lambda i, h: rows.at[1, :, span(h), at_x(i)], x, to_x),
        )
        made = [
            Gather(b, i, to, ag_s.at[4 * k + n], ag_r.at[4 * k + n])
            for n, (b, i, to) in enumerate(blocks)
        ]
        return made[:2], made[2:]

    def expert(k):
        span = pl.ds(k * chunk, chunk)
        deep = rows.shape[3]
        hidden = jnp.zeros((chunk, 2 * COLS), F32)
        d_act = jnp.zeros((chunk, COLS), F32)
        for j in range(SIDE):
            hidden += dot(rows[0, j, span, :], wide[j * deep : (j + 1) * deep, :], 1, 0)
            d_act += dot(rows[1, j, span, :], down_w[:, j * deep : (j + 1) * deep], 1, 1)
        gate_pre, up_pre = hidden[:, :COLS], hidden[:, COLS:]
        sigma = jax.nn.sigmoid(gate_pre)
        swish = gate_pre * sigma
        act[span, :] = (swish * up_pre).astype(BF16)
        d_wide[span, :COLS] = (
            d_act * up_pre * sigma * (1.0 + gate_pre * (1.0 - sigma))
        ).astype(BF16)
        d_wide[span, COLS:] = (d_act * swish).astype(BF16)
        for j in range(SIDE):
            for i in range(0, SIDE, 2):
                low = (j * SIDE + i) * COLS
                piece = dot(d_wide[span, :], wide[low : low + 2 * COLS, :], 1, 1).astype(BF16)
                part[j, i, span, :] = piece[:, :COLS]
                part[j, i + 1, span, :] = piece[:, COLS:]

    def scatters(k):
        base, half, quarter = k * chunk, chunk // 2, chunk // 4

        def span(start, h):
            return pl.ds(start + h * quarter, quarter)

        def full(buf, n):
            return lambda h: buf.at[n, :, pl.ds(h * quarter, quarter), :]

        def flat(buf, n):
            return lambda h: buf.at[n, pl.ds(h * quarter, quarter), :]

        n = 2 * k
        made = (
            Scatter(
                lambda i, h: part.at[:, i, span(base, h), :], x, to_x,
                rs_s.at[4 * k], rs_r.at[4 * k],
                lambda h: t_buf.at[n, h], full(lo_buf, n), full(hi_buf, n),
            ),
            Scatter(
                lambda i, h: part.at[i, :, span(base + half, h), :], y, to_y,
                rs_s.at[4 * k + 1], rs_r.at[4 * k + 1],
                lambda h: t_buf.at[n + 1, h], full(lo_buf, n + 1), full(hi_buf, n + 1),
            ),
            Scatter(
                lambda i, h: s_buf.at[n, i, pl.ds(h * quarter, quarter), :], y, to_y,
                rs_s.at[4 * k + 2], rs_r.at[4 * k + 2],
                lambda h: t2_buf.at[n, h], flat(lo2_buf, n), flat(hi2_buf, n),
            ),
            Scatter(
                lambda i, h: s_buf.at[n + 1, i, pl.ds(h * quarter, quarter), :], x, to_x,
                rs_s.at[4 * k + 3], rs_r.at[4 * k + 3],
                lambda h: t2_buf.at[n + 1, h], flat(lo2_buf, n + 1), flat(hi2_buf, n + 1),
            ),
        )
        return made[:2], made[2:]

    def between(k, first):
        quarter = chunk // 4
        for n, ring in enumerate(first):
            for h in (0, 1):
                s_buf[2 * k + n, :, pl.ds(h * quarter, quarter), :] = ring.total(h).astype(BF16)

    def give_back(k, second):
        half, quarter = chunk // 2, chunk // 4
        for n, ring in enumerate(second):
            for h in (0, 1):
                back[pl.ds(k * chunk + n * half + h * quarter, quarter), :] = ring.total(h).astype(
                    BF16
                )
        dst = arrived.at[pl.ds(pl.multiple_of(sp * CAP, CAP), CAP), :]
        for d, c in others[::-1]:
            pos = place(-d)
            if (pos < near) != (k == 0):
                continue
            where = rows_at(pos, 1 - core if d == 0 else c)
            send(back.at[where, :], dst, back_s.at[k], back_r, to_sp(other(d, c)))
        if k == 0:
            pltpu.make_async_copy(back.at[rows_at(SHIFT, core), :], dst, back_r).start()

    def each(rings, name, label=""):
        with jax.named_scope(label + name):
            for ring in rings:
                getattr(ring, name)()

    a0, b0 = gathers(0)
    a1, b1 = gathers(1)
    r0, q0 = scatters(0)
    r1, q1 = scatters(1)

    z_arrived(0)
    each(a0, "first", "a0_")
    each(a0, "relay", "a0_")
    each(a0, "last", "a0_")
    each(b0, "first", "b0_")
    z_arrived(1)
    each(a1, "first", "a1_")
    each(b0, "relay", "b0_")
    each(a1, "relay", "a1_")
    each(b0, "last", "b0_")
    each(a1, "last", "a1_")
    each(b1, "first", "b1_")
    have(9, 15)
    with jax.named_scope("expert0"):
        expert(0)
    each(r0, "first", "r0_")
    each(b1, "relay", "b1_")
    each(r0, "relay", "r0_")
    each(r0, "last", "r0_")
    between(0, r0)
    each(q0, "first", "q0_")
    each(b1, "last", "b1_")
    with jax.named_scope("expert1"):
        expert(1)
    each(r1, "first", "r1_")
    each(q0, "relay", "q0_")
    each(q0, "last", "q0_")
    give_back(0, q0)
    each(r1, "relay", "r1_")
    each(r1, "last", "r1_")
    between(1, r1)
    each(q1, "first", "q1_")
    each(q1, "relay", "q1_")
    each(q1, "last", "q1_")
    give_back(1, q1)

    with jax.named_scope("grads"):
        deep = rows.shape[3]
        for j in range(SIDE):
            grads = dot(rows[0, j], d_wide[...], 0, 0).astype(BF16)
            g_gate[j * deep : (j + 1) * deep, :] = grads[:, :COLS]
            g_up[j * deep : (j + 1) * deep, :] = grads[:, COLS:]
            g_down[:, j * deep : (j + 1) * deep] = dot(act[...], rows[1, j], 0, 0).astype(BF16)
        stored = (
            pltpu.make_async_copy(g_gate, g_gate_h.at[0], g_s.at[0]),
            pltpu.make_async_copy(g_up, g_up_h.at[0], g_s.at[1]),
            pltpu.make_async_copy(g_down, g_down_h.at[0], g_s.at[2]),
        )
        for copy in stored:
            copy.start()

    with jax.named_scope("lead_wait"):
        take(leads.at[pl.ds(0, ns - 1)], lead_r)
    state_in = jnp.zeros((1, channels), F32)
    for i in range(ns):
        v = leads[i]
        state_in = jnp.where(i < sp, v[:, :channels] * state_in + v[:, channels:], state_in)
    run = jnp.ones((1, channels), F32)
    for i in range(ns):
        coef[i] = jnp.where(i > sp, run, 0.0)
        run = jnp.where(i > sp, run * leads[i][:, :channels], run)
    state_in = standing(state_in)
    state = rows_f[1] + rows_f[0] * state_in
    rows_f[6] = (moved(state, 1, state_in) * rows_f[2] - rows_f[6]) * rows_f[7]
    hidden = state.astype(BF16)

    with jax.named_scope("back_wait"):
        take(arrived, back_r)
    dn[y, :, own_x] = dot(picked[...], arrived[...], 0, 0).astype(BF16)
    half = tokens // 2

    def spot(n, i, j):
        return dn.at[j, pl.ds(n * half, half), pl.ds(pl.multiple_of(i * COLS, COLS), COLS)]

    def spread(n, i, j, along_x, slot):
        ref = spot(n, i, j)
        for v in (2, 1, 3):
            target = to_x(lax.rem(x + v, SIDE)) if along_x else to_y(lax.rem(y + v, SIDE))
            send(ref, ref, dn_s.at[n, slot, v - 1], dn_r.at[n, slot, v - 1], target)

    def back_by(p, v):
        return lax.rem(p + SIDE - v, SIDE)

    for n in (0, 1):
        spread(n, x, y, n == 0, 0)
    for n in (0, 1):
        spread(n, x, y, n == 1, 1)
    with jax.named_scope("dn_first"):
        for v in (1, 3, 2):
            for n in (0, 1):
                i, j = (back_by(x, v), y) if n == 0 else (x, back_by(y, v))
                take(spot(n, i, j), dn_r.at[n, 0, v - 1])
                spread(n, i, j, n == 1, 1 + v)
    with jax.named_scope("dn_last"):
        for v in (0, 1, 3, 2):
            for w in (1, 3, 2):
                for n in (0, 1):
                    i, j = (
                        (back_by(x, v), back_by(y, w)) if n == 0 else (back_by(x, w), back_by(y, v))
                    )
                    take(spot(n, i, j), dn_r.at[n, 1 + v, w - 1])

    with jax.named_scope("mix"):
        inv_rms = upright(irms[...])
        stat = jnp.zeros((tokens, 1), F32)
        for j in range(SIDE):
            cols = pl.ds(j * deep, deep)
            g = gain[:, cols]
            stat += jnp.sum(
                (g * dn[j].astype(F32)) * (norm[:, cols].astype(F32) / g), axis=1, keepdims=True
            )
        stat = stat / norm.shape[1]
        for j in range(SIDE):
            cols = pl.ds(j * deep, deep)
            g = gain[:, cols]
            mix = cot[:, cols].astype(F32) + inv_rms * (
                g * dn[j].astype(F32) - (norm[:, cols].astype(F32) / g) * stat
            )
            d_mix[:, cols] = mix.astype(BF16)

    with jax.named_scope("trail"):
        d_state = dot(out_m[...], d_mix[...], 1, 1)
        tail, grad_loc = scan(rows_f[3], d_state, -1)
        first_grad = lying(rows_f[2][:, :1] * grad_loc[:, :1])
        trail[...] = jnp.concatenate([first_grad, first_grad], axis=1)
        trails[sp] = trail[...]
        for d, c in others:
            send(trail, trails.at[sp], trail_s, trail_r, to_sp(other(d, c)))

    with jax.named_scope("gw_dot"):
        wide_piece = 2 * g_out.shape[0]
        gw = dot(hidden, d_mix[...], 1, 0)
        for n in range(nz):
            band = gw[:, n * wide_piece : (n + 1) * wide_piece]
            top, low = band[: channels // 2, :], band[channels // 2 :, :]
            cut = g_out.shape[0]
            gw_all[0, n] = jnp.concatenate([top[:, :cut], low[:, :cut]], axis=1).astype(BF16)
            gw_all[1, n] = jnp.concatenate([top[:, cut:], low[:, cut:]], axis=1).astype(BF16)

    send(gw_all.at[1 - core], gw_pair, pair_s, pair_r, to_sp(z * 2 + 1 - core))
    with jax.named_scope("pair_wait"):
        take(gw_pair, pair_r)
    gw_chip[...] = (gw_all[core].astype(F32) + gw_pair[...].astype(F32)).astype(BF16)
    for d in steps[::-1]:
        zz = lax.rem(z + d + nz, nz)
        send(gw_chip.at[zz], gw_in.at[z], gw_s, gw_r, to_sp(zz * 2 + core))
    pltpu.make_async_copy(gw_chip.at[z], gw_in.at[z], gw_r).start()
    with jax.named_scope("trail_wait"):
        take(trails.at[pl.ds(0, ns - 1)], trail_r)
    entering = jnp.zeros((1, channels), F32)
    for i in range(ns):
        entering += coef[i] * trails[i][:, :channels]
    total = grad_loc + tail * standing(entering)
    g_rec[...] = total * rows_f[4]
    g_in[...] = total * rows_f[5]
    g_dec[...] = total * rows_f[6]
    with jax.named_scope("gw_wait"):
        take(gw_in, gw_r)
    acc = jnp.zeros(gw_in.shape[1:], F32)
    for i in range(nz):
        acc += gw_in[i].astype(F32)
    cut = g_out.shape[0]
    g_out[...] = jnp.concatenate([acc[:, :cut], acc[:, cut:]], axis=0).T

    for copy in stored:
        copy.wait()
    block = ns // 2 * CAP
    take(packed.at[:, pl.ds(0, block - CAP), :], z_s.at[0])
    take(packed.at[:, pl.ds(0, block), :], z_s.at[1])
    for ring in a0 + b0 + a1 + b1 + list(r0) + list(q0) + list(r1) + list(q1):
        ring.sent()
    for n in (0, 1):
        for slot in range(5):
            for v in range(3):
                take(spot(n, x, y), dn_s.at[n, slot, v])
    take(back.at[pl.ds(0, block - CAP), :], back_s.at[0])
    take(back.at[pl.ds(0, block), :], back_s.at[1])
    take(leads.at[pl.ds(0, ns - 1)], lead_s)
    take(trails.at[pl.ds(0, ns - 1)], trail_s)
    take(gw_pair, pair_s)
    take(gw_in.at[pl.ds(0, nz - 1)], gw_s)


def finish(count, *refs):
    held, came, left = refs[2 * count : 3 * count], refs[-2], refs[-1]
    into = [pltpu.make_async_copy(refs[n], held[n], came.at[n]) for n in range(count)]
    out = [pltpu.make_async_copy(held[n], refs[count + n], left.at[n]) for n in range(count)]
    for copy in into:
        copy.start()
    for first, second in zip(into, out):
        first.wait()
        second.start()
    for copy in out:
        copy.wait()


def shards(
    cotangent,
    normed,
    inverse_root_mean_square,
    expert_norm_scale,
    routes,
    route_probability_weight,
    gate_weight,
    up_weight,
    down_weight,
    recurrence_input,
    recurrence_gate_logits,
    input_gate_logits,
    channel_decay_weight,
    extra_log_decay,
    output_matrix,
):
    ns = lax.axis_size("sp")
    tokens, features = normed.shape
    channels = recurrence_input.shape[1]
    slots = ns * CAP
    chunk, quarter = slots // 2, slots // 8
    wide = features // SIDE
    vmem, dma = pltpu.VMEM, pltpu.SemaphoreType.DMA
    args = (
        cotangent,
        normed,
        inverse_root_mean_square.reshape(1, tokens),
        expert_norm_scale.reshape(1, features),
        routes.T,
        route_probability_weight.T,
        gate_weight,
        up_weight,
        down_weight,
        recurrence_input.T,
        recurrence_gate_logits.T,
        input_gate_logits.T,
        channel_decay_weight.reshape(1, channels),
        extra_log_decay.T,
        output_matrix.T,
    )
    f32_rows = jax.ShapeDtypeStruct((channels, tokens), F32)
    vm, hbm = pl.BlockSpec(memory_space=pltpu.VMEM), pl.BlockSpec(memory_space=pl.ANY)
    results = pl.pallas_call(
        functools.partial(kernel, ns),
        out_shape=(
            jax.ShapeDtypeStruct(gate_weight.shape, BF16),
            jax.ShapeDtypeStruct(up_weight.shape, BF16),
            jax.ShapeDtypeStruct(down_weight.shape, BF16),
            jax.ShapeDtypeStruct((features // ns, channels), F32),
            f32_rows,
            f32_rows,
            f32_rows,
        ),
        in_specs=[hbm] * len(args),
        out_specs=[hbm] * 3 + [vm] * 4,
        scratch_shapes=[
            vmem((2, slots, COLS), BF16),
            vmem((slots, tokens), BF16),
            vmem((2, SIDE, slots, wide), BF16),
            vmem((features, 2 * COLS), BF16),
            vmem((slots, 2 * COLS), BF16),
            vmem((slots, COLS), BF16),
            vmem((SIDE, SIDE, slots, COLS), BF16),
            vmem((4, 2, SIDE, quarter, COLS), BF16),
            vmem((4, SIDE, 2 * quarter, COLS), BF16),
            vmem((4, SIDE, 2 * quarter, COLS), BF16),
            vmem((4, SIDE, 2 * quarter, COLS), BF16),
            vmem((4, 2, quarter, COLS), BF16),
            vmem((4, 2 * quarter, COLS), BF16),
            vmem((4, 2 * quarter, COLS), BF16),
            vmem((slots, COLS), BF16),
            vmem((slots, COLS), BF16),
            vmem((SIDE, tokens, wide), BF16),
            vmem((tokens, features), BF16),
            vmem((8, channels, tokens), F32),
            vmem((1, 2 * channels), F32),
            vmem((ns, 1, 2 * channels), F32),
            vmem((1, 2 * channels), F32),
            vmem((ns, 1, 2 * channels), F32),
            vmem((ns, 1, channels), F32),
            vmem((2, ns // 2, features // ns // 2, 2 * channels), BF16),
            vmem((ns // 2, features // ns // 2, 2 * channels), BF16),
            vmem((ns // 2, features // ns // 2, 2 * channels), BF16),
            vmem((ns // 2, features // ns // 2, 2 * channels), BF16),
            vmem((COLS, features), BF16),
            vmem((features, COLS), BF16),
            vmem((features, COLS), BF16),
            vmem((COLS, features), BF16),
            *(vmem(args[n].shape, args[n].dtype) for n in (0, 1, 2, 3, 4, 5)),
            *(vmem(a.shape, a.dtype) for a in args[9:]),
            dma((len(args),)),
            dma((3,)),
            dma((2,)),
            dma((2,)),
            dma((8, 4)),
            dma((8, 4)),
            dma((8, 6)),
            dma((8, 6)),
            dma((2, 5, 3)),
            dma((2, 5, 3)),
            dma((2,)),
            dma,
            dma,
            dma,
            dma,
            dma,
            dma,
            dma,
            dma,
            dma,
        ],
        compiler_params=pltpu.CompilerParams(
            collective_id=0, has_side_effects=True, vmem_limit_bytes=FULL
        ),
    )(*args)
    g_gate, g_up, g_down, g_out, g_rec, g_dec, g_in = pl.pallas_call(
        functools.partial(finish, len(results)),
        out_shape=tuple(jax.ShapeDtypeStruct(r.shape, r.dtype) for r in results),
        in_specs=[hbm] * len(results),
        out_specs=[hbm] * len(results),
        scratch_shapes=[vmem(r.shape, r.dtype) for r in results]
        + [dma((len(results),)), dma((len(results),))],
        compiler_params=pltpu.CompilerParams(vmem_limit_bytes=FULL),
    )(*results)
    return g_gate, g_up, g_down, g_out, g_rec.T, g_dec.T, g_in.T


def solution(mesh):
    placed = (
        P("sp", None),
        P("sp", None),
        P("sp"),
        P(),
        P("sp", None),
        P("sp", None),
        P("sp", None, "tp"),
        P("sp", None, "tp"),
        P("sp", "tp", None),
        P("sp", "tp"),
        P("sp", "tp"),
        P("sp", "tp"),
        P("tp"),
        P("sp", "tp"),
        P(None, "tp"),
    )
    return jax.shard_map(
        shards,
        mesh=mesh,
        in_specs=placed,
        out_specs=(
            P("sp", None, "tp"),
            P("sp", None, "tp"),
            P("sp", "tp", None),
            P("sp", "tp"),
            P("sp", "tp"),
            P("sp", "tp"),
            P("sp", "tp"),
        ),
        check_vma=False,
    )
```

```python
import functools

import jax
import jax.numpy as jnp
from jax import lax
from jax.experimental import pallas as pl
from jax.experimental.pallas import tpu as pltpu
from jax.sharding import PartitionSpec as P

MESH = pl.DeviceIdType.MESH
F32 = jnp.float32
BF16 = jnp.bfloat16
SIDE = 4
CHUNKS = (4, 6, 4, 2)
COLS = 128
ORDER = (('begin', 0), ('near', 0), ('relay', 0, 0), ('begin', 1), ('across', 0), ('relay', 0, 2), ('relay', 0, 1), ('near', 1), ('relay', 1, 0), ('relay', 0, 3), ('begin', 2), ('across', 1), ('relay', 1, 2), ('relay', 1, 1), ('begin', 3), ('expert', 0), ('near', 2), ('relay', 2, 0), ('relay', 1, 3), ('near', 3), ('relay', 3, 0), ('mid', 0), ('across', 2), ('relay', 2, 2), ('relay', 2, 1), ('expert', 1), ('across', 3), ('relay', 3, 2), ('relay', 3, 1), ('turn', 0), ('relay', 2, 3), ('mid', 1), ('relay', 3, 3), ('expert', 2), ('give', 0), ('turn', 1), ('expert', 3), ('mid', 2), ('give', 1), ('mid', 3), ('turn', 2), ('turn', 3), ('give', 2), ('give', 3))
FIRST_EXPERT = [step for step, *_ in ORDER].index("expert")
CAP = 16
FULL = 67_043_328


def dot(a, b, ca, cb):
    return lax.dot_general(a, b, (((ca,), (cb,)), ((), ())), preferred_element_type=F32)


def take(ref, sem):
    pltpu.make_async_copy(ref, ref, sem).wait()


def send(src, dst, send_sem, recv_sem, target):
    pltpu.make_async_remote_copy(
        src_ref=src,
        dst_ref=dst,
        send_sem=send_sem,
        recv_sem=recv_sem,
        device_id=target,
        device_id_type=MESH,
    ).start()


class Flow:
    def __init__(self, piece, bulk, p, q, to_p, to_q, ss, rs):
        self.piece, self.bulk, self.p, self.q, self.to_p, self.to_q, self.ss, self.rs = (
            piece, bulk, p, q, to_p, to_q, ss, rs,
        )
        self.from_p = [p] + [lax.rem(p + SIDE - v, SIDE) for v in (1, 3, 2)]

    def along_p(self, ref, v, k):
        send(ref, ref, self.ss, self.rs.at[k], self.to_p(lax.rem(self.p + v, SIDE)))

    def along_q(self, ref, v, k):
        send(ref, ref, self.ss, self.rs.at[k], self.to_q(lax.rem(self.q + v, SIDE)))

    def mine(self, m, half=None):
        return self.piece(self.from_p[m], self.q, half)

    def other(self, m, v, half=None):
        return self.piece(self.from_p[m], lax.rem(self.q + SIDE - v, SIDE), half)

    def cross(self, m):
        self.along_q(self.mine(m), 1, 3 + m)
        self.along_q(self.mine(m), 3, 3 + m)

    def start(self):
        self.along_p(self.mine(0), 1, 0)
        self.along_p(self.mine(0), 3, 0)
        self.cross(0)

    def near(self):
        take(self.bulk(2), self.rs.at[0])
        self.along_p(self.mine(1, 0), 1, 1)
        self.along_p(self.mine(2, 1), 3, 1)
        self.cross(1)
        self.cross(2)

    def across(self):
        take(self.bulk(1), self.rs.at[1])
        self.cross(3)

    def relay(self, m):
        take(self.bulk(2), self.rs.at[3 + m])
        self.along_q(self.other(m, 1, 0), 1, 2)
        self.along_q(self.other(m, 3, 1), 3, 2)

    def last(self):
        take(self.bulk(SIDE), self.rs.at[2])


class Scatter:
    def __init__(self, block, i, axis_to, ss, rs, part, came, parts, all_came):
        self.block, self.i, self.to, self.ss, self.rs = block, i, axis_to, ss, rs
        self.part, self.came, self.parts, self.all_came = part, came, parts, all_came
        self.up, self.down, self.far = lax.rem(i + 1, 4), lax.rem(i + 3, 4), lax.rem(i + 2, 4)

    def go(self, src, dst, target, k):
        send(src, dst, self.ss, self.rs.at[k], target)

    def first(self):
        up, down = self.to(self.up), self.to(self.down)
        self.go(self.block(self.far, 0), self.part(0), up, 0)
        self.go(self.block(self.far, 1), self.part(1), down, 0)
        self.go(self.block(self.up, 1), self.came(0, 1), up, 1)
        self.go(self.block(self.down, 0), self.came(1, 0), down, 1)

    def relay(self):
        take(self.parts, self.rs.at[0])
        for member, half, dst in (
            (self.up, 0, self.came(0, 0)),
            (self.down, 1, self.came(1, 1)),
        ):
            ref = self.block(member, half)
            ref[...] = (ref[...].astype(F32) + self.part(half)[...].astype(F32)).astype(BF16)
            self.go(ref, dst, self.to(member), 1)

    def last(self):
        take(self.all_came, self.rs.at[1])

    def total(self, half):
        return (
            self.block(self.i, half)[...].astype(F32)
            + self.came(0, half)[...].astype(F32)
            + self.came(1, half)[...].astype(F32)
        )


class Direct:
    def __init__(self, block, i, axis_to, ss, rs, slot, slots):
        self.block, self.i, self.to, self.ss, self.rs = block, i, axis_to, ss, rs
        self.slot, self.slots = slot, slots

    def first(self):
        for v in (2, 1, 3):
            target = lax.rem(self.i + v, SIDE)
            send(self.block(target), self.slot(v - 1), self.ss, self.rs, self.to(target))

    def total(self):
        take(self.slots, self.rs)
        value = self.block(self.i)[...].astype(F32)
        for v in range(SIDE - 1):
            value += self.slot(v)[...].astype(F32)
        return value


def softplus(v):
    z = jnp.exp(-jnp.abs(v))
    s = z / (2.0 + z)
    q = s * s
    series = jnp.zeros_like(s)
    for k in range(9, -1, -1):
        series = series * q + 1.0 / (2 * k + 1)
    return jnp.maximum(v, 0.0) + 2.0 * s * series


def expm1(v):
    near = jnp.clip(v, -0.5, 0.5)
    series = jnp.ones_like(v)
    for k in range(10, 1, -1):
        series = 1.0 + near * series * (1.0 / k)
    return jnp.where(jnp.abs(v) < 0.5, near * series, jnp.exp(v) - 1.0)


def kernel(
    ns,
    cot_h,
    norm_h,
    irms_h,
    gain_h,
    routes_h,
    prob_h,
    gate_h,
    up_h,
    down_h,
    rec_in_h,
    rec_gate_h,
    in_gate_h,
    decay_h,
    extra_h,
    out_h,
    g_gate_h,
    g_up_h,
    g_down_h,
    g_out,
    g_rec,
    g_dec,
    g_in,
    packed,
    picked,
    rows,
    wide,
    d_wide,
    act,
    part,
    t_buf,
    c_buf,
    s_buf,
    t2_buf,
    back,
    arrived,
    dn,
    d_mix,
    rows_f,
    powers,
    lead,
    leads,
    trail,
    trails,
    coef,
    gw_all,
    gw_pair,
    gw_chip,
    gw_in,
    down_w,
    g_gate,
    g_up,
    g_down,
    cot,
    norm,
    irms,
    gain,
    routes,
    prob,
    rec_in,
    rec_gate,
    in_gate,
    decay_w,
    extra,
    out_m,
    w_r,
    g_s,
    z_s,
    z_r,
    ag_s,
    ag_r,
    rs_s,
    rs_r,
    dn_s,
    dn_r,
    back_s,
    back_r,
    lead_s,
    lead_r,
    trail_s,
    trail_r,
    pair_s,
    pair_r,
    gw_s,
    gw_r,
):
    sp, tp = lax.axis_index("sp"), lax.axis_index("tp")
    z, core = lax.div(sp, 2), lax.rem(sp, 2)
    y, x = lax.div(tp, SIDE), lax.rem(tp, SIDE)
    nz = ns // 2
    tokens = norm.shape[0]
    first_chip = [sum(CHUNKS[:k]) for k in range(len(CHUNKS) + 1)]
    row_count = [n * 2 * CAP for n in CHUNKS]
    row_base = [n * 2 * CAP for n in first_chip]
    by_distance = [0] + [d for v in range(1, nz // 2) for d in (v, -v)] + [nz // 2]

    def place(d):
        return by_distance.index(d)

    def chunk_of(pos):
        return sum(pos >= first for first in first_chip[1:-1])

    def to_x(v):
        return {"sp": sp, "tp": y * SIDE + v}

    def to_y(v):
        return {"sp": sp, "tp": v * SIDE + x}

    def to_sp(v):
        return {"sp": v, "tp": tp}

    barrier = pltpu.get_barrier_semaphore()
    steps = by_distance[1:]
    others = [(0, 1)] + [(d, c) for d in steps for c in (0, 1)]

    def other(d, c):
        if d == 0:
            return z * 2 + (1 - core)
        return lax.rem(z + d + nz, nz) * 2 + c

    for d, c in others:
        pl.semaphore_signal(barrier, inc=1, device_id=to_sp(other(d, c)), device_id_type=MESH)
    for v in (1, 3):
        pl.semaphore_signal(
            barrier, inc=1, device_id=to_x(lax.rem(x + v, SIDE)), device_id_type=MESH
        )
        pl.semaphore_signal(
            barrier, inc=1, device_id=to_y(lax.rem(y + v, SIDE)), device_id_type=MESH
        )

    moves = (
        (routes_h, routes),
        (prob_h, prob),
        (norm_h, norm),
        (cot_h, cot),
        (rec_gate_h, rec_gate),
        (in_gate_h, in_gate),
        (rec_in_h, rec_in),
        (decay_h, decay_w),
        (extra_h, extra),
        (gate_h.at[0], wide.at[:, :COLS]),
        (up_h.at[0], wide.at[:, COLS:]),
        (down_h.at[0], down_w),
        (irms_h, irms),
        (gain_h, gain),
        (out_h, out_m),
    )
    moves = [pltpu.make_async_copy(a, b, w_r.at[k]) for k, (a, b) in enumerate(moves)]
    for copy in moves:
        copy.start()

    def have(first, last):
        for copy in moves[first:last]:
            copy.wait()

    mine = pl.ds(pl.multiple_of(tp * COLS, COLS), COLS)
    def eye(n):
        return lax.broadcasted_iota(jnp.int32, (n, n), 0) == lax.broadcasted_iota(
            jnp.int32, (n, n), 1
        )

    square = eye(tokens)

    def upright(row):
        return jnp.sum(jnp.where(square, row, 0.0), axis=1, keepdims=True)

    have(0, 4)
    expert_id = lax.broadcasted_iota(jnp.int32, (ns, tokens), 0)
    chosen = [routes[k : k + 1, :] for k in (0, 1)]
    member = [(e == expert_id).astype(F32) for e in chosen]
    earlier = (
        lax.broadcasted_iota(jnp.int32, (tokens, tokens), 0)
        < lax.broadcasted_iota(jnp.int32, (tokens, tokens), 1)
    ).astype(BF16)
    before = dot((member[0] + member[1]).astype(BF16), earlier, 1, 0)
    slot = lax.broadcasted_iota(jnp.int32, (ns * CAP, tokens), 0).astype(F32)
    one = [
        (slot == (e.astype(F32) * CAP + jnp.sum(m * before, axis=0, keepdims=True))).astype(F32)
        for e, m in zip(chosen, member)
    ]
    both = (one[0] + one[1]).astype(BF16)
    picked[...] = both
    own_cot = cot[:, mine].astype(F32)
    packed[0] = dot(both, norm[:, mine], 1, 0).astype(BF16)
    packed[1] = (
        dot(one[0].astype(BF16), (upright(prob[0:1, :]) * own_cot).astype(BF16), 1, 0)
        + dot(one[1].astype(BF16), (upright(prob[1:2, :]) * own_cot).astype(BF16), 1, 0)
    ).astype(BF16)

    with jax.named_scope("barrier"):
        pl.semaphore_wait(barrier, len(others) + 4)

    own_x = pl.ds(pl.multiple_of(x * COLS, COLS), COLS)

    def rows_at(pos, c):
        return pl.ds(pl.multiple_of((pos * 2 + c) * CAP, CAP), CAP)

    by_chunk = [[p for p in others if chunk_of(place(p[0])) == k] for k in range(len(CHUNKS))]
    for k, (d, c) in [(k, p) for k, pairs in enumerate(by_chunk) for p in pairs[::-1]]:
        target = other(d, c)
        send(
            packed.at[:, pl.ds(pl.multiple_of(target * CAP, CAP), CAP), :],
            rows.at[:, y, rows_at(place(d), core), own_x],
            z_s,
            z_r.at[k],
            to_sp(target),
        )
    pltpu.make_async_copy(
        packed.at[:, pl.ds(pl.multiple_of(sp * CAP, CAP), CAP), :],
        rows.at[:, y, rows_at(0, core), own_x],
        z_r.at[0],
    ).start()

    channels = extra.shape[0]
    corner = eye(channels)

    def lying(column):
        return jnp.sum(jnp.where(corner, column, 0.0), axis=0, keepdims=True)

    def standing(row):
        return jnp.sum(jnp.where(corner, row, 0.0), axis=1, keepdims=True)

    token = lax.broadcasted_iota(jnp.int32, (channels, tokens), 1)

    def moved(v, step, fill):
        inside = token >= step if step > 0 else token < tokens + step
        return jnp.where(inside, pltpu.roll(v, step % tokens, 1), fill)

    levels = tokens.bit_length() - 1

    def scan(a, b, sign):
        step = 1
        while step < tokens:
            b = a * moved(b, sign * step, 0.0) + b
            a = a * moved(a, sign * step, 1.0)
            step *= 2
        return a, b

    with jax.named_scope("recur"):
        have(4, 9)
        retain = jax.nn.sigmoid(rec_gate[...].astype(F32))
        admit = jax.nn.sigmoid(in_gate[...].astype(F32))
        signal = rec_in[...].astype(F32)
        speed = standing(-8.0 * softplus(-decay_w[...]))
        log_keep = retain * speed + extra[...]
        keep = jnp.exp(log_keep)
        scale_in = jnp.sqrt(-expm1(2.0 * log_keep))
        keep_cum, state_loc = scan(keep, scale_in * admit * signal, 1)
        lead[...] = jnp.concatenate(
            [lying(keep_cum[:, tokens - 1 :]), lying(state_loc[:, tokens - 1 :])], axis=1
        )
        leads[sp] = lead[...]
        for d, c in others:
            send(lead, leads.at[sp], lead_s, lead_r, to_sp(other(d, c)))
        rows_f[0] = keep_cum
        rows_f[1] = state_loc
        rows_f[2] = keep
        tail = moved(keep, -1, 1.0)
        for level in range(levels):
            powers[level] = tail
            tail = tail * moved(tail, -(1 << level), 1.0)
        rows_f[3] = tail
        rows_f[4] = scale_in * admit
        rows_f[5] = scale_in * signal * admit * (1.0 - admit)
        rows_f[6] = admit * signal * keep * keep / scale_in
        rows_f[7] = speed * retain * (1.0 - retain)

    def z_arrived(k):
        take(rows.at[:, y, pl.ds(row_base[k], row_count[k]), own_x], z_r.at[k])

    def at_x(i):
        return pl.ds(pl.multiple_of(i * COLS, COLS), COLS)

    def flows(k):
        half_rows = row_count[k] // 2

        def span(half):
            if half is None:
                return pl.ds(row_base[k], row_count[k])
            return pl.ds(row_base[k] + half * half_rows, half_rows)

        def bulk(count):
            return rows.at[0, pl.ds(0, count), span(None), pl.ds(0, COLS)]

        return (
            Flow(
                lambda p, q, h: rows.at[0, q, span(h), at_x(p)],
                bulk, x, y, to_x, to_y, ag_s, ag_r.at[2 * k],
            ),
            Flow(
                lambda p, q, h: rows.at[1, p, span(h), at_x(q)],
                bulk, y, x, to_y, to_x, ag_s, ag_r.at[2 * k + 1],
            ),
        )

    def expert(k):
        chunk = row_count[k]
        span = pl.ds(row_base[k], chunk)
        deep = rows.shape[3]
        hidden = jnp.zeros((chunk, 2 * COLS), F32)
        d_act = jnp.zeros((chunk, COLS), F32)
        for j in range(SIDE):
            hidden += dot(rows[0, j, span, :], wide[j * deep : (j + 1) * deep, :], 1, 0)
            d_act += dot(rows[1, j, span, :], down_w[:, j * deep : (j + 1) * deep], 1, 1)
        gate_pre, up_pre = hidden[:, :COLS], hidden[:, COLS:]
        sigma = jax.nn.sigmoid(gate_pre)
        swish = gate_pre * sigma
        act[span, :] = (swish * up_pre).astype(BF16)
        d_wide[span, :COLS] = (
            d_act * up_pre * sigma * (1.0 + gate_pre * (1.0 - sigma))
        ).astype(BF16)
        d_wide[span, COLS:] = (d_act * swish).astype(BF16)
        for j in range(SIDE):
            for i in range(0, SIDE, 2):
                low = (j * SIDE + i) * COLS
                piece = dot(d_wide[span, :], wide[low : low + 2 * COLS, :], 1, 1).astype(BF16)
                part[j, i, span, :] = piece[:, :COLS]
                part[j, i + 1, span, :] = piece[:, COLS:]

    def scatters(k):
        base, half, quarter = row_base[k], row_count[k] // 2, row_count[k] // 4

        def span(start, h):
            return pl.ds(start + h * quarter, quarter)

        def make(n, block, i, axis_to, i2, axis_to2):
            one = Scatter(
                block, i, axis_to, rs_s.at[0], rs_r.at[n],
                lambda h: t_buf.at[n, h, :, pl.ds(0, quarter), :],
                lambda v, h: c_buf.at[n, v, :, pl.ds(h * quarter, quarter), :],
                t_buf.at[n, :, :, pl.ds(0, quarter), :],
                c_buf.at[n, :, :, pl.ds(0, half), :],
            )
            two = Direct(
                lambda m: s_buf.at[n, m, pl.ds(0, half), :], i2, axis_to2,
                rs_s.at[1], rs_r.at[n, 2],
                lambda v: t2_buf.at[n, v, pl.ds(0, half), :],
                t2_buf.at[n, :, pl.ds(0, half), :],
            )
            return one, two

        a1, a2 = make(
            2 * k, lambda i, h: part.at[:, i, span(base, h), :], x, to_x, y, to_y
        )
        b1, b2 = make(
            2 * k + 1, lambda i, h: part.at[i, :, span(base + half, h), :], y, to_y, x, to_x
        )
        return (a1, b1), (a2, b2)

    def between(k, first):
        quarter = row_count[k] // 4
        for n, ring in enumerate(first):
            for h in (0, 1):
                s_buf[2 * k + n, :, pl.ds(h * quarter, quarter), :] = ring.total(h).astype(BF16)

    def give_back(k, second):
        half = row_count[k] // 2
        for n, ring in enumerate(second):
            back[pl.ds(row_base[k] + n * half, half), :] = ring.total().astype(BF16)
        dst = arrived.at[pl.ds(pl.multiple_of(sp * CAP, CAP), CAP), :]
        for d, c in others[::-1]:
            pos = place(-d if 0 < abs(d) < nz // 2 else d)
            if chunk_of(pos) != k:
                continue
            where = rows_at(pos, 1 - core if d == 0 else c)
            send(back.at[where, :], dst, back_s, back_r, to_sp(other(d, c)))
        if k == 0:
            pltpu.make_async_copy(back.at[rows_at(0, core), :], dst, back_r).start()

    all_flows = [flows(k) for k in range(len(CHUNKS))]
    all_sums = [scatters(k) for k in range(len(CHUNKS))]

    def both_of(pair, name, *given):
        for one_of in pair:
            getattr(one_of, name)(*given)

    for number, (step, k, *given) in enumerate(ORDER):
        with jax.named_scope(f"{step}{k}" + "".join(f"_{m}" for m in given)):
            if step == "begin":
                z_arrived(k)
                both_of(all_flows[k], "start")
            elif step == "expert":
                if number == FIRST_EXPERT:
                    have(9, 15)
                both_of(all_flows[k], "last")
                expert(k)
                both_of(all_sums[k][0], "first")
            elif step == "mid":
                both_of(all_sums[k][0], "relay")
            elif step == "turn":
                both_of(all_sums[k][0], "last")
                between(k, all_sums[k][0])
                both_of(all_sums[k][1], "first")
            elif step == "give":
                give_back(k, all_sums[k][1])
            else:
                both_of(all_flows[k], step, *given)

    with jax.named_scope("grads"):
        deep = rows.shape[3]
        for j in range(SIDE):
            grads = dot(rows[0, j], d_wide[...], 0, 0).astype(BF16)
            g_gate[j * deep : (j + 1) * deep, :] = grads[:, :COLS]
            g_up[j * deep : (j + 1) * deep, :] = grads[:, COLS:]
            g_down[:, j * deep : (j + 1) * deep] = dot(act[...], rows[1, j], 0, 0).astype(BF16)
        stored = (
            pltpu.make_async_copy(g_gate, g_gate_h.at[0], g_s.at[0]),
            pltpu.make_async_copy(g_up, g_up_h.at[0], g_s.at[1]),
            pltpu.make_async_copy(g_down, g_down_h.at[0], g_s.at[2]),
        )
        for copy in stored:
            copy.start()

    with jax.named_scope("sent"):
        all_rows = ns * CAP
        take(packed.at[:, pl.ds(0, all_rows - CAP), :], z_s)
        take(rows.at[:, :, pl.ds(0, all_rows // 16 * 15), :], ag_s)
        take(part.at[pl.ds(0, 3)], rs_s.at[0])
        take(part.at[0, pl.ds(0, 3)], rs_s.at[1])
        take(back.at[pl.ds(0, all_rows - CAP), :], back_s)
        take(leads.at[pl.ds(0, ns - 1)], lead_s)

    with jax.named_scope("lead_wait"):
        take(leads.at[pl.ds(0, ns - 1)], lead_r)
    state_in = jnp.zeros((1, channels), F32)
    for i in range(ns):
        v = leads[i]
        state_in = jnp.where(i < sp, v[:, :channels] * state_in + v[:, channels:], state_in)
    run = jnp.ones((1, channels), F32)
    for i in range(ns):
        coef[i] = jnp.where(i > sp, run, 0.0)
        run = jnp.where(i > sp, run * leads[i][:, :channels], run)
    state_in = standing(state_in)
    state = rows_f[1] + rows_f[0] * state_in
    rows_f[6] = (moved(state, 1, state_in) * rows_f[2] - rows_f[6]) * rows_f[7]
    hidden = state.astype(BF16)

    with jax.named_scope("back_wait"):
        take(arrived, back_r)
    dn[y, :, own_x] = dot(picked[...], arrived[...], 0, 0).astype(BF16)
    half = tokens // 2

    def spot(n, i, j):
        return dn.at[j, pl.ds(n * half, half), pl.ds(pl.multiple_of(i * COLS, COLS), COLS)]

    def spread(n, i, j, along_x, slot):
        ref = spot(n, i, j)
        for v in (2, 1, 3):
            target = to_x(lax.rem(x + v, SIDE)) if along_x else to_y(lax.rem(y + v, SIDE))
            send(ref, ref, dn_s, dn_r.at[n, v - 1 if slot == 0 else 3], target)

    def back_by(p, v):
        return lax.rem(p + SIDE - v, SIDE)

    for n in (0, 1):
        spread(n, x, y, n == 0, 0)
    for n in (0, 1):
        spread(n, x, y, n == 1, 1)
    with jax.named_scope("dn_first"):
        for v in (1, 3, 2):
            for n in (0, 1):
                i, j = (back_by(x, v), y) if n == 0 else (x, back_by(y, v))
                take(spot(n, i, j), dn_r.at[n, v - 1])
                spread(n, i, j, n == 1, 1 + v)
    with jax.named_scope("dn_last"):
        for n in (0, 1):
            take(dn.at[pl.ds(0, 3), pl.ds(0, half), :], dn_r.at[n, 3])

    with jax.named_scope("mix"):
        inv_rms = upright(irms[...])
        stat = jnp.zeros((tokens, 1), F32)
        for j in range(SIDE):
            cols = pl.ds(j * deep, deep)
            g = gain[:, cols]
            stat += jnp.sum(
                (g * dn[j].astype(F32)) * (norm[:, cols].astype(F32) / g), axis=1, keepdims=True
            )
        stat = stat / norm.shape[1]
        for j in range(SIDE):
            cols = pl.ds(j * deep, deep)
            g = gain[:, cols]
            mix = cot[:, cols].astype(F32) + inv_rms * (
                g * dn[j].astype(F32) - (norm[:, cols].astype(F32) / g) * stat
            )
            d_mix[:, cols] = mix.astype(BF16)

    with jax.named_scope("gw_dot"):
        wide_piece = 2 * g_out.shape[0]
        gw = dot(hidden, d_mix[...], 1, 0)
        for n in range(nz):
            band = gw[:, n * wide_piece : (n + 1) * wide_piece]
            top, low = band[: channels // 2, :], band[channels // 2 :, :]
            cut = g_out.shape[0]
            gw_all[0, n] = jnp.concatenate([top[:, :cut], low[:, :cut]], axis=1).astype(BF16)
            gw_all[1, n] = jnp.concatenate([top[:, cut:], low[:, cut:]], axis=1).astype(BF16)

    send(gw_all.at[1 - core], gw_pair, pair_s, pair_r, to_sp(z * 2 + 1 - core))
    with jax.named_scope("trail"):
        d_state = dot(out_m[...], d_mix[...], 1, 1)
        grad_loc = d_state
        for level in range(levels):
            grad_loc += powers[level] * moved(grad_loc, -(1 << level), 0.0)
        first_grad = lying(rows_f[2][:, :1] * grad_loc[:, :1])
        trail[...] = jnp.concatenate([first_grad, first_grad], axis=1)
        trails[sp] = trail[...]
        for d, c in others:
            send(trail, trails.at[sp], trail_s, trail_r, to_sp(other(d, c)))

    with jax.named_scope("pair_wait"):
        take(gw_pair, pair_r)
    gw_chip[...] = (gw_all[core].astype(F32) + gw_pair[...].astype(F32)).astype(BF16)
    for d in steps[::-1]:
        zz = lax.rem(z + d + nz, nz)
        send(gw_chip.at[zz], gw_in.at[z], gw_s, gw_r, to_sp(zz * 2 + core))
    pltpu.make_async_copy(gw_chip.at[z], gw_in.at[z], gw_r).start()
    take(rows.at[0, 0, pl.ds(0, rows.shape[2] // 16 * 15), :], dn_s)
    for copy in stored:
        copy.wait()
    with jax.named_scope("trail_wait"):
        take(trails.at[pl.ds(0, ns - 1)], trail_r)
    entering = jnp.zeros((1, channels), F32)
    for i in range(ns):
        entering += coef[i] * trails[i][:, :channels]
    total = grad_loc + rows_f[3] * standing(entering)
    g_rec[...] = total * rows_f[4]
    g_in[...] = total * rows_f[5]
    g_dec[...] = total * rows_f[6]
    with jax.named_scope("gw_wait"):
        take(gw_in, gw_r)
    acc = jnp.zeros(gw_in.shape[1:], F32)
    for i in range(nz):
        acc += gw_in[i].astype(F32)
    cut = g_out.shape[0]
    g_out[...] = jnp.concatenate([acc[:, :cut], acc[:, cut:]], axis=0).T

    take(trails.at[pl.ds(0, ns - 1)], trail_s)
    take(gw_pair, pair_s)
    take(gw_in.at[pl.ds(0, nz - 1)], gw_s)


def finish(count, *refs):
    held, came, left = refs[2 * count : 3 * count], refs[-2], refs[-1]
    into = [pltpu.make_async_copy(refs[n], held[n], came.at[n]) for n in range(count)]
    out = [pltpu.make_async_copy(held[n], refs[count + n], left.at[n]) for n in range(count)]
    for copy in into:
        copy.start()
    for first, second in zip(into, out):
        first.wait()
        second.start()
    for copy in out:
        copy.wait()


def shards(
    cotangent,
    normed,
    inverse_root_mean_square,
    expert_norm_scale,
    routes,
    route_probability_weight,
    gate_weight,
    up_weight,
    down_weight,
    recurrence_input,
    recurrence_gate_logits,
    input_gate_logits,
    channel_decay_weight,
    extra_log_decay,
    output_matrix,
):
    ns = lax.axis_size("sp")
    tokens, features = normed.shape
    channels = recurrence_input.shape[1]
    slots = ns * CAP
    chunks = len(CHUNKS)
    quarter = max(CHUNKS) * 2 * CAP // 4
    wide = features // SIDE
    vmem, dma = pltpu.VMEM, pltpu.SemaphoreType.DMA
    args = (
        cotangent,
        normed,
        inverse_root_mean_square.reshape(1, tokens),
        expert_norm_scale.reshape(1, features),
        routes.T,
        route_probability_weight.T,
        gate_weight,
        up_weight,
        down_weight,
        recurrence_input.T,
        recurrence_gate_logits.T,
        input_gate_logits.T,
        channel_decay_weight.reshape(1, channels),
        extra_log_decay.T,
        output_matrix.T,
    )
    f32_rows = jax.ShapeDtypeStruct((channels, tokens), F32)
    vm, hbm = pl.BlockSpec(memory_space=pltpu.VMEM), pl.BlockSpec(memory_space=pl.ANY)
    results = pl.pallas_call(
        functools.partial(kernel, ns),
        out_shape=(
            jax.ShapeDtypeStruct(gate_weight.shape, BF16),
            jax.ShapeDtypeStruct(up_weight.shape, BF16),
            jax.ShapeDtypeStruct(down_weight.shape, BF16),
            jax.ShapeDtypeStruct((features // ns, channels), F32),
            f32_rows,
            f32_rows,
            f32_rows,
        ),
        in_specs=[hbm] * len(args),
        out_specs=[hbm] * 3 + [vm] * 4,
        scratch_shapes=[
            vmem((2, slots, COLS), BF16),
            vmem((slots, tokens), BF16),
            vmem((2, SIDE, slots, wide), BF16),
            vmem((features, 2 * COLS), BF16),
            vmem((slots, 2 * COLS), BF16),
            vmem((slots, COLS), BF16),
            vmem((SIDE, SIDE, slots, COLS), BF16),
            vmem((2 * chunks, 2, SIDE, quarter, COLS), BF16),
            vmem((2 * chunks, 2, SIDE, 2 * quarter, COLS), BF16),
            vmem((2 * chunks, SIDE, 2 * quarter, COLS), BF16),
            vmem((2 * chunks, 3, 2 * quarter, COLS), BF16),
            vmem((slots, COLS), BF16),
            vmem((slots, COLS), BF16),
            vmem((SIDE, tokens, wide), BF16),
            vmem((tokens, features), BF16),
            vmem((8, channels, tokens), F32),
            vmem((tokens.bit_length() - 1, channels, tokens), F32),
            vmem((1, 2 * channels), F32),
            vmem((ns, 1, 2 * channels), F32),
            vmem((1, 2 * channels), F32),
            vmem((ns, 1, 2 * channels), F32),
            vmem((ns, 1, channels), F32),
            vmem((2, ns // 2, features // ns // 2, 2 * channels), BF16),
            vmem((ns // 2, features // ns // 2, 2 * channels), BF16),
            vmem((ns // 2, features // ns // 2, 2 * channels), BF16),
            vmem((ns // 2, features // ns // 2, 2 * channels), BF16),
            vmem((COLS, features), BF16),
            vmem((features, COLS), BF16),
            vmem((features, COLS), BF16),
            vmem((COLS, features), BF16),
            *(vmem(args[n].shape, args[n].dtype) for n in (0, 1, 2, 3, 4, 5)),
            *(vmem(a.shape, a.dtype) for a in args[9:]),
            dma((len(args),)),
            dma((3,)),
            dma,
            dma((chunks,)),
            dma,
            dma((2 * chunks, 7)),
            dma((2,)),
            dma((2 * chunks, 3)),
            dma,
            dma((2, 4)),
            dma,
            dma,
            dma,
            dma,
            dma,
            dma,
            dma,
            dma,
            dma,
            dma,
        ],
        compiler_params=pltpu.CompilerParams(
            collective_id=0, has_side_effects=True, vmem_limit_bytes=FULL
        ),
    )(*args)
    g_gate, g_up, g_down, g_out, g_rec, g_dec, g_in = pl.pallas_call(
        functools.partial(finish, len(results)),
        out_shape=tuple(jax.ShapeDtypeStruct(r.shape, r.dtype) for r in results),
        in_specs=[hbm] * len(results),
        out_specs=[hbm] * len(results),
        scratch_shapes=[vmem(r.shape, r.dtype) for r in results]
        + [dma((len(results),)), dma((len(results),))],
        compiler_params=pltpu.CompilerParams(vmem_limit_bytes=FULL),
    )(*results)
    return g_gate, g_up, g_down, g_out, g_rec.T, g_dec.T, g_in.T


def solution(mesh):
    placed = (
        P("sp", None),
        P("sp", None),
        P("sp"),
        P(),
        P("sp", None),
        P("sp", None),
        P("sp", None, "tp"),
        P("sp", None, "tp"),
        P("sp", "tp", None),
        P("sp", "tp"),
        P("sp", "tp"),
        P("sp", "tp"),
        P("tp"),
        P("sp", "tp"),
        P(None, "tp"),
    )
    return jax.shard_map(
        shards,
        mesh=mesh,
        in_specs=placed,
        out_specs=(
            P("sp", None, "tp"),
            P("sp", None, "tp"),
            P("sp", "tp", None),
            P("sp", "tp"),
            P("sp", "tp"),
            P("sp", "tp"),
            P("sp", "tp"),
        ),
        check_vma=False,
    )
```

```python
import functools

import jax
import jax.numpy as jnp
from jax import lax
from jax.experimental import pallas as pl
from jax.experimental.pallas import tpu as pltpu
from jax.sharding import PartitionSpec as P

MESH = pl.DeviceIdType.MESH
F32 = jnp.float32
BF16 = jnp.bfloat16
SIDE = 4
CHUNKS = (4, 6, 4, 2)
SOURCES = (1, -1, 2, -2, 4, -4, 5, -5, 6, -6, 7, -7, 8, 3, 0, -3)
COLS = 128
ORDER = (('begin', 0), ('near', 0), ('relay', 0, 0), ('begin', 1), ('across', 0), ('relay', 0, 2), ('relay', 0, 1), ('near', 1), ('relay', 1, 0), ('relay', 0, 3), ('begin', 2), ('across', 1), ('relay', 1, 2), ('relay', 1, 1), ('begin', 3), ('expert', 0), ('near', 2), ('relay', 2, 0), ('relay', 1, 3), ('near', 3), ('relay', 3, 0), ('mid', 0), ('across', 2), ('relay', 2, 2), ('relay', 2, 1), ('expert', 1), ('across', 3), ('relay', 3, 2), ('relay', 3, 1), ('turn', 0), ('relay', 2, 3), ('mid', 1), ('relay', 3, 3), ('expert', 2), ('give', 0), ('turn', 1), ('expert', 3), ('mid', 2), ('give', 1), ('mid', 3), ('turn', 2), ('turn', 3), ('give', 2), ('give', 3))
FIRST_EXPERT = [step for step, *_ in ORDER].index("expert")
CAP = 16
FULL = 67_043_328


def dot(a, b, ca, cb):
    return lax.dot_general(a, b, (((ca,), (cb,)), ((), ())), preferred_element_type=F32)


def take(ref, sem):
    pltpu.make_async_copy(ref, ref, sem).wait()


def send(src, dst, send_sem, recv_sem, target):
    pltpu.make_async_remote_copy(
        src_ref=src,
        dst_ref=dst,
        send_sem=send_sem,
        recv_sem=recv_sem,
        device_id=target,
        device_id_type=MESH,
    ).start()


class Flow:
    def __init__(self, piece, bulk, p, q, to_p, to_q, ss, rs):
        self.piece, self.bulk, self.p, self.q, self.to_p, self.to_q, self.ss, self.rs = (
            piece, bulk, p, q, to_p, to_q, ss, rs,
        )
        self.from_p = [p] + [lax.rem(p + SIDE - v, SIDE) for v in (1, 3, 2)]

    def along_p(self, ref, v, k):
        send(ref, ref, self.ss, self.rs.at[k], self.to_p(lax.rem(self.p + v, SIDE)))

    def along_q(self, ref, v, k):
        send(ref, ref, self.ss, self.rs.at[k], self.to_q(lax.rem(self.q + v, SIDE)))

    def mine(self, m, half=None):
        return self.piece(self.from_p[m], self.q, half)

    def other(self, m, v, half=None):
        return self.piece(self.from_p[m], lax.rem(self.q + SIDE - v, SIDE), half)

    def cross(self, m):
        self.along_q(self.mine(m), 1, 3 + m)
        self.along_q(self.mine(m), 3, 3 + m)

    def start(self):
        self.along_p(self.mine(0), 1, 0)
        self.along_p(self.mine(0), 3, 0)
        self.cross(0)

    def near(self):
        take(self.bulk(2), self.rs.at[0])
        self.along_p(self.mine(1, 0), 1, 1)
        self.along_p(self.mine(2, 1), 3, 1)
        self.cross(1)
        self.cross(2)

    def across(self):
        take(self.bulk(1), self.rs.at[1])
        self.cross(3)

    def relay(self, m):
        take(self.bulk(2), self.rs.at[3 + m])
        self.along_q(self.other(m, 1, 0), 1, 2)
        self.along_q(self.other(m, 3, 1), 3, 2)

    def last(self):
        take(self.bulk(SIDE), self.rs.at[2])


class Scatter:
    def __init__(self, block, i, axis_to, ss, rs, part, came, parts, all_came):
        self.block, self.i, self.to, self.ss, self.rs = block, i, axis_to, ss, rs
        self.part, self.came, self.parts, self.all_came = part, came, parts, all_came
        self.up, self.down, self.far = lax.rem(i + 1, 4), lax.rem(i + 3, 4), lax.rem(i + 2, 4)

    def go(self, src, dst, target, k):
        send(src, dst, self.ss, self.rs.at[k], target)

    def first(self):
        up, down = self.to(self.up), self.to(self.down)
        self.go(self.block(self.far, 0), self.part(0), up, 0)
        self.go(self.block(self.far, 1), self.part(1), down, 0)
        self.go(self.block(self.up, 1), self.came(0, 1), up, 1)
        self.go(self.block(self.down, 0), self.came(1, 0), down, 1)

    def relay(self):
        take(self.parts, self.rs.at[0])
        for member, half, dst in (
            (self.up, 0, self.came(0, 0)),
            (self.down, 1, self.came(1, 1)),
        ):
            ref = self.block(member, half)
            ref[...] = (ref[...].astype(F32) + self.part(half)[...].astype(F32)).astype(BF16)
            self.go(ref, dst, self.to(member), 1)

    def last(self):
        take(self.all_came, self.rs.at[1])

    def total(self, half):
        return (
            self.block(self.i, half)[...].astype(F32)
            + self.came(0, half)[...].astype(F32)
            + self.came(1, half)[...].astype(F32)
        )


class Direct:
    def __init__(self, block, i, axis_to, ss, rs, slot, slots):
        self.block, self.i, self.to, self.ss, self.rs = block, i, axis_to, ss, rs
        self.slot, self.slots = slot, slots

    def first(self):
        for v in (2, 1, 3):
            target = lax.rem(self.i + v, SIDE)
            send(self.block(target), self.slot(v - 1), self.ss, self.rs, self.to(target))

    def total(self):
        take(self.slots, self.rs)
        value = self.block(self.i)[...].astype(F32)
        for v in range(SIDE - 1):
            value += self.slot(v)[...].astype(F32)
        return value


def softplus(v):
    z = jnp.exp(-jnp.abs(v))
    s = z / (2.0 + z)
    q = s * s
    series = jnp.zeros_like(s)
    for k in range(9, -1, -1):
        series = series * q + 1.0 / (2 * k + 1)
    return jnp.maximum(v, 0.0) + 2.0 * s * series


def expm1(v):
    near = jnp.clip(v, -0.5, 0.5)
    series = jnp.ones_like(v)
    for k in range(10, 1, -1):
        series = 1.0 + near * series * (1.0 / k)
    return jnp.where(jnp.abs(v) < 0.5, near * series, jnp.exp(v) - 1.0)


def kernel(
    ns,
    cot_h,
    norm_h,
    irms_h,
    gain_h,
    routes_h,
    prob_h,
    gate_h,
    up_h,
    down_h,
    rec_in_h,
    rec_gate_h,
    in_gate_h,
    decay_h,
    extra_h,
    out_h,
    g_gate_h,
    g_up_h,
    g_down_h,
    g_out,
    g_rec,
    g_dec,
    g_in,
    packed,
    picked,
    rows,
    wide,
    d_wide,
    act,
    part,
    t_buf,
    c_buf,
    s_buf,
    t2_buf,
    back,
    arrived,
    dn,
    d_mix,
    rows_f,
    powers,
    lead,
    leads,
    trail,
    trails,
    coef,
    gw_all,
    gw_pair,
    gw_chip,
    gw_in,
    down_w,
    g_gate,
    g_up,
    g_down,
    cot,
    norm,
    irms,
    gain,
    routes,
    prob,
    rec_in,
    rec_gate,
    in_gate,
    decay_w,
    extra,
    out_m,
    w_r,
    g_s,
    z_s,
    z_r,
    ag_s,
    ag_r,
    rs_s,
    rs_r,
    dn_s,
    dn_r,
    back_s,
    back_r,
    lead_s,
    lead_r,
    trail_s,
    trail_r,
    pair_s,
    pair_r,
    gw_s,
    gw_r,
):
    sp, tp = lax.axis_index("sp"), lax.axis_index("tp")
    z, core = lax.div(sp, 2), lax.rem(sp, 2)
    y, x = lax.div(tp, SIDE), lax.rem(tp, SIDE)
    nz = ns // 2
    tokens = norm.shape[0]
    first_chip = [sum(CHUNKS[:k]) for k in range(len(CHUNKS) + 1)]
    row_count = [n * 2 * CAP for n in CHUNKS]
    row_base = [n * 2 * CAP for n in first_chip]
    home = SOURCES.index(0)

    def place(d):
        return SOURCES.index(d)

    def chunk_of(pos):
        return sum(pos >= first for first in first_chip[1:-1])

    def to_x(v):
        return {"sp": sp, "tp": y * SIDE + v}

    def to_y(v):
        return {"sp": sp, "tp": v * SIDE + x}

    def to_sp(v):
        return {"sp": v, "tp": tp}

    barrier = pltpu.get_barrier_semaphore()
    steps = [d for d in SOURCES if d != 0]
    others = [(d, c) for d in SOURCES for c in (0, 1) if (d, c) != (0, 0)]

    def other(d, c):
        if d == 0:
            return z * 2 + (1 - core)
        return lax.rem(z + d + nz, nz) * 2 + c

    for d, c in others:
        pl.semaphore_signal(barrier, inc=1, device_id=to_sp(other(d, c)), device_id_type=MESH)
    for v in (1, 3):
        pl.semaphore_signal(
            barrier, inc=1, device_id=to_x(lax.rem(x + v, SIDE)), device_id_type=MESH
        )
        pl.semaphore_signal(
            barrier, inc=1, device_id=to_y(lax.rem(y + v, SIDE)), device_id_type=MESH
        )

    moves = (
        (routes_h, routes),
        (prob_h, prob),
        (norm_h, norm),
        (cot_h, cot),
        (rec_gate_h, rec_gate),
        (in_gate_h, in_gate),
        (rec_in_h, rec_in),
        (decay_h, decay_w),
        (extra_h, extra),
        (gate_h.at[0], wide.at[:, :COLS]),
        (up_h.at[0], wide.at[:, COLS:]),
        (down_h.at[0], down_w),
        (irms_h, irms),
        (gain_h, gain),
        (out_h, out_m),
    )
    moves = [pltpu.make_async_copy(a, b, w_r.at[k]) for k, (a, b) in enumerate(moves)]
    for copy in moves:
        copy.start()

    def have(first, last):
        for copy in moves[first:last]:
            copy.wait()

    mine = pl.ds(pl.multiple_of(tp * COLS, COLS), COLS)
    def eye(n):
        return lax.broadcasted_iota(jnp.int32, (n, n), 0) == lax.broadcasted_iota(
            jnp.int32, (n, n), 1
        )

    square = eye(tokens)

    def upright(row):
        return jnp.sum(jnp.where(square, row, 0.0), axis=1, keepdims=True)

    have(0, 4)
    expert_id = lax.broadcasted_iota(jnp.int32, (ns, tokens), 0)
    chosen = [routes[k : k + 1, :] for k in (0, 1)]
    member = [(e == expert_id).astype(F32) for e in chosen]
    earlier = (
        lax.broadcasted_iota(jnp.int32, (tokens, tokens), 0)
        < lax.broadcasted_iota(jnp.int32, (tokens, tokens), 1)
    ).astype(BF16)
    before = dot((member[0] + member[1]).astype(BF16), earlier, 1, 0)
    slot = lax.broadcasted_iota(jnp.int32, (ns * CAP, tokens), 0).astype(F32)
    one = [
        (slot == (e.astype(F32) * CAP + jnp.sum(m * before, axis=0, keepdims=True))).astype(F32)
        for e, m in zip(chosen, member)
    ]
    both = (one[0] + one[1]).astype(BF16)
    picked[...] = both
    own_cot = cot[:, mine].astype(F32)
    packed[0] = dot(both, norm[:, mine], 1, 0).astype(BF16)
    packed[1] = (
        dot(one[0].astype(BF16), (upright(prob[0:1, :]) * own_cot).astype(BF16), 1, 0)
        + dot(one[1].astype(BF16), (upright(prob[1:2, :]) * own_cot).astype(BF16), 1, 0)
    ).astype(BF16)

    with jax.named_scope("barrier"):
        pl.semaphore_wait(barrier, len(others) + 4)

    own_x = pl.ds(pl.multiple_of(x * COLS, COLS), COLS)

    def rows_at(pos, c):
        return pl.ds(pl.multiple_of((pos * 2 + c) * CAP, CAP), CAP)

    by_chunk = [[p for p in others if chunk_of(place(p[0])) == k] for k in range(len(CHUNKS))]
    for k, (d, c) in [(k, p) for k, pairs in enumerate(by_chunk) for p in pairs[::-1]]:
        target = other(d, c)
        send(
            packed.at[:, pl.ds(pl.multiple_of(target * CAP, CAP), CAP), :],
            rows.at[:, y, rows_at(place(d), core), own_x],
            z_s,
            z_r.at[k],
            to_sp(target),
        )
    pltpu.make_async_copy(
        packed.at[:, pl.ds(pl.multiple_of(sp * CAP, CAP), CAP), :],
        rows.at[:, y, rows_at(home, core), own_x],
        z_r.at[chunk_of(home)],
    ).start()

    channels = extra.shape[0]
    corner = eye(channels)

    def lying(column):
        return jnp.sum(jnp.where(corner, column, 0.0), axis=0, keepdims=True)

    def standing(row):
        return jnp.sum(jnp.where(corner, row, 0.0), axis=1, keepdims=True)

    token = lax.broadcasted_iota(jnp.int32, (channels, tokens), 1)

    def moved(v, step, fill):
        inside = token >= step if step > 0 else token < tokens + step
        return jnp.where(inside, pltpu.roll(v, step % tokens, 1), fill)

    levels = tokens.bit_length() - 1

    def scan(a, b, sign):
        step = 1
        while step < tokens:
            b = a * moved(b, sign * step, 0.0) + b
            a = a * moved(a, sign * step, 1.0)
            step *= 2
        return a, b

    with jax.named_scope("recur"):
        have(4, 9)
        retain = jax.nn.sigmoid(rec_gate[...].astype(F32))
        admit = jax.nn.sigmoid(in_gate[...].astype(F32))
        signal = rec_in[...].astype(F32)
        speed = standing(-8.0 * softplus(-decay_w[...]))
        log_keep = retain * speed + extra[...]
        keep = jnp.exp(log_keep)
        scale_in = jnp.sqrt(-expm1(2.0 * log_keep))
        keep_cum, state_loc = scan(keep, scale_in * admit * signal, 1)
        lead[...] = jnp.concatenate(
            [lying(keep_cum[:, tokens - 1 :]), lying(state_loc[:, tokens - 1 :])], axis=1
        )
        leads[sp] = lead[...]
        for d, c in others:
            send(lead, leads.at[sp], lead_s, lead_r, to_sp(other(d, c)))
        rows_f[0] = keep_cum
        rows_f[1] = state_loc
        rows_f[2] = keep
        tail = moved(keep, -1, 1.0)
        for level in range(levels):
            powers[level] = tail
            tail = tail * moved(tail, -(1 << level), 1.0)
        rows_f[3] = tail
        rows_f[4] = scale_in * admit
        rows_f[5] = scale_in * signal * admit * (1.0 - admit)
        rows_f[6] = admit * signal * keep * keep / scale_in
        rows_f[7] = speed * retain * (1.0 - retain)

    def z_arrived(k):
        take(rows.at[:, y, pl.ds(row_base[k], row_count[k]), own_x], z_r.at[k])

    def at_x(i):
        return pl.ds(pl.multiple_of(i * COLS, COLS), COLS)

    def flows(k):
        half_rows = row_count[k] // 2

        def span(half):
            if half is None:
                return pl.ds(row_base[k], row_count[k])
            return pl.ds(row_base[k] + half * half_rows, half_rows)

        def bulk(count):
            return rows.at[0, pl.ds(0, count), span(None), pl.ds(0, COLS)]

        return (
            Flow(
                lambda p, q, h: rows.at[0, q, span(h), at_x(p)],
                bulk, x, y, to_x, to_y, ag_s, ag_r.at[2 * k],
            ),
            Flow(
                lambda p, q, h: rows.at[1, p, span(h), at_x(q)],
                bulk, y, x, to_y, to_x, ag_s, ag_r.at[2 * k + 1],
            ),
        )

    def expert(k):
        chunk = row_count[k]
        span = pl.ds(row_base[k], chunk)
        deep = rows.shape[3]
        hidden = jnp.zeros((chunk, 2 * COLS), F32)
        d_act = jnp.zeros((chunk, COLS), F32)
        for j in range(SIDE):
            hidden += dot(rows[0, j, span, :], wide[j * deep : (j + 1) * deep, :], 1, 0)
            d_act += dot(rows[1, j, span, :], down_w[:, j * deep : (j + 1) * deep], 1, 1)
        gate_pre, up_pre = hidden[:, :COLS], hidden[:, COLS:]
        sigma = jax.nn.sigmoid(gate_pre)
        swish = gate_pre * sigma
        act[span, :] = (swish * up_pre).astype(BF16)
        d_wide[span, :COLS] = (
            d_act * up_pre * sigma * (1.0 + gate_pre * (1.0 - sigma))
        ).astype(BF16)
        d_wide[span, COLS:] = (d_act * swish).astype(BF16)
        for j in range(SIDE):
            for i in range(0, SIDE, 2):
                low = (j * SIDE + i) * COLS
                piece = dot(d_wide[span, :], wide[low : low + 2 * COLS, :], 1, 1).astype(BF16)
                part[j, i, span, :] = piece[:, :COLS]
                part[j, i + 1, span, :] = piece[:, COLS:]

    def scatters(k):
        base, half, quarter = row_base[k], row_count[k] // 2, row_count[k] // 4

        def span(start, h):
            return pl.ds(start + h * quarter, quarter)

        def make(n, block, i, axis_to, i2, axis_to2):
            one = Scatter(
                block, i, axis_to, rs_s.at[0], rs_r.at[n],
                lambda h: t_buf.at[n, h, :, pl.ds(0, quarter), :],
                lambda v, h: c_buf.at[n, v, :, pl.ds(h * quarter, quarter), :],
                t_buf.at[n, :, :, pl.ds(0, quarter), :],
                c_buf.at[n, :, :, pl.ds(0, half), :],
            )
            two = Direct(
                lambda m: s_buf.at[n, m, pl.ds(0, half), :], i2, axis_to2,
                rs_s.at[1], rs_r.at[n, 2],
                lambda v: t2_buf.at[n, v, pl.ds(0, half), :],
                t2_buf.at[n, :, pl.ds(0, half), :],
            )
            return one, two

        a1, a2 = make(
            2 * k, lambda i, h: part.at[:, i, span(base, h), :], x, to_x, y, to_y
        )
        b1, b2 = make(
            2 * k + 1, lambda i, h: part.at[i, :, span(base + half, h), :], y, to_y, x, to_x
        )
        return (a1, b1), (a2, b2)

    def between(k, first):
        quarter = row_count[k] // 4
        for n, ring in enumerate(first):
            for h in (0, 1):
                s_buf[2 * k + n, :, pl.ds(h * quarter, quarter), :] = ring.total(h).astype(BF16)

    def give_back(k, second):
        half = row_count[k] // 2
        for n, ring in enumerate(second):
            back[pl.ds(row_base[k] + n * half, half), :] = ring.total().astype(BF16)
        dst = arrived.at[pl.ds(pl.multiple_of(sp * CAP, CAP), CAP), :]
        for d, c in others[::-1]:
            pos = place(-d if 0 < abs(d) < nz // 2 else d)
            if chunk_of(pos) != k:
                continue
            where = rows_at(pos, 1 - core if d == 0 else c)
            send(back.at[where, :], dst, back_s, back_r, to_sp(other(d, c)))
        if k == chunk_of(home):
            pltpu.make_async_copy(back.at[rows_at(home, core), :], dst, back_r).start()

    all_flows = [flows(k) for k in range(len(CHUNKS))]
    all_sums = [scatters(k) for k in range(len(CHUNKS))]

    def both_of(pair, name, *given):
        for one_of in pair:
            getattr(one_of, name)(*given)

    for number, (step, k, *given) in enumerate(ORDER):
        with jax.named_scope(f"{step}{k}" + "".join(f"_{m}" for m in given)):
            if step == "begin":
                z_arrived(k)
                both_of(all_flows[k], "start")
            elif step == "expert":
                if number == FIRST_EXPERT:
                    have(9, 15)
                both_of(all_flows[k], "last")
                expert(k)
                both_of(all_sums[k][0], "first")
            elif step == "mid":
                both_of(all_sums[k][0], "relay")
            elif step == "turn":
                both_of(all_sums[k][0], "last")
                between(k, all_sums[k][0])
                both_of(all_sums[k][1], "first")
            elif step == "give":
                give_back(k, all_sums[k][1])
            else:
                both_of(all_flows[k], step, *given)

    with jax.named_scope("grads"):
        deep = rows.shape[3]
        for j in range(SIDE):
            grads = dot(rows[0, j], d_wide[...], 0, 0).astype(BF16)
            g_gate[j * deep : (j + 1) * deep, :] = grads[:, :COLS]
            g_up[j * deep : (j + 1) * deep, :] = grads[:, COLS:]
            g_down[:, j * deep : (j + 1) * deep] = dot(act[...], rows[1, j], 0, 0).astype(BF16)
        stored = (
            pltpu.make_async_copy(g_gate, g_gate_h.at[0], g_s.at[0]),
            pltpu.make_async_copy(g_up, g_up_h.at[0], g_s.at[1]),
            pltpu.make_async_copy(g_down, g_down_h.at[0], g_s.at[2]),
        )
        for copy in stored:
            copy.start()

    with jax.named_scope("sent"):
        all_rows = ns * CAP
        take(packed.at[:, pl.ds(0, all_rows - CAP), :], z_s)
        take(rows.at[:, :, pl.ds(0, all_rows // 16 * 15), :], ag_s)
        take(part.at[pl.ds(0, 3)], rs_s.at[0])
        take(part.at[0, pl.ds(0, 3)], rs_s.at[1])
        take(back.at[pl.ds(0, all_rows - CAP), :], back_s)
        take(leads.at[pl.ds(0, ns - 1)], lead_s)

    with jax.named_scope("lead_wait"):
        take(leads.at[pl.ds(0, ns - 1)], lead_r)
    state_in = jnp.zeros((1, channels), F32)
    for i in range(ns):
        v = leads[i]
        state_in = jnp.where(i < sp, v[:, :channels] * state_in + v[:, channels:], state_in)
    run = jnp.ones((1, channels), F32)
    for i in range(ns):
        coef[i] = jnp.where(i > sp, run, 0.0)
        run = jnp.where(i > sp, run * leads[i][:, :channels], run)
    state_in = standing(state_in)
    state = rows_f[1] + rows_f[0] * state_in
    rows_f[6] = (moved(state, 1, state_in) * rows_f[2] - rows_f[6]) * rows_f[7]
    hidden = state.astype(BF16)

    with jax.named_scope("back_wait"):
        take(arrived, back_r)
    dn[y, :, own_x] = dot(picked[...], arrived[...], 0, 0).astype(BF16)
    half = tokens // 2

    def spot(n, i, j):
        return dn.at[j, pl.ds(n * half, half), pl.ds(pl.multiple_of(i * COLS, COLS), COLS)]

    def spread(n, i, j, along_x, slot):
        ref = spot(n, i, j)
        for v in (2, 1, 3):
            target = to_x(lax.rem(x + v, SIDE)) if along_x else to_y(lax.rem(y + v, SIDE))
            send(ref, ref, dn_s, dn_r.at[n, v - 1 if slot == 0 else 3], target)

    def back_by(p, v):
        return lax.rem(p + SIDE - v, SIDE)

    for n in (0, 1):
        spread(n, x, y, n == 0, 0)
    for n in (0, 1):
        spread(n, x, y, n == 1, 1)
    with jax.named_scope("dn_first"):
        for v in (1, 3, 2):
            for n in (0, 1):
                i, j = (back_by(x, v), y) if n == 0 else (x, back_by(y, v))
                take(spot(n, i, j), dn_r.at[n, v - 1])
                spread(n, i, j, n == 1, 1 + v)
    with jax.named_scope("dn_last"):
        for n in (0, 1):
            take(dn.at[pl.ds(0, 3), pl.ds(0, half), :], dn_r.at[n, 3])

    with jax.named_scope("mix"):
        inv_rms = upright(irms[...])
        stat = jnp.zeros((tokens, 1), F32)
        for j in range(SIDE):
            cols = pl.ds(j * deep, deep)
            g = gain[:, cols]
            stat += jnp.sum(
                (g * dn[j].astype(F32)) * (norm[:, cols].astype(F32) / g), axis=1, keepdims=True
            )
        stat = stat / norm.shape[1]
        for j in range(SIDE):
            cols = pl.ds(j * deep, deep)
            g = gain[:, cols]
            mix = cot[:, cols].astype(F32) + inv_rms * (
                g * dn[j].astype(F32) - (norm[:, cols].astype(F32) / g) * stat
            )
            d_mix[:, cols] = mix.astype(BF16)

    with jax.named_scope("gw_dot"):
        wide_piece = 2 * g_out.shape[0]
        gw = dot(hidden, d_mix[...], 1, 0)
        for n in range(nz):
            band = gw[:, n * wide_piece : (n + 1) * wide_piece]
            top, low = band[: channels // 2, :], band[channels // 2 :, :]
            cut = g_out.shape[0]
            gw_all[0, n] = jnp.concatenate([top[:, :cut], low[:, :cut]], axis=1).astype(BF16)
            gw_all[1, n] = jnp.concatenate([top[:, cut:], low[:, cut:]], axis=1).astype(BF16)

    send(gw_all.at[1 - core], gw_pair, pair_s, pair_r, to_sp(z * 2 + 1 - core))
    with jax.named_scope("trail"):
        d_state = dot(out_m[...], d_mix[...], 1, 1)
        grad_loc = d_state
        for level in range(levels):
            grad_loc += powers[level] * moved(grad_loc, -(1 << level), 0.0)
        first_grad = lying(rows_f[2][:, :1] * grad_loc[:, :1])
        trail[...] = jnp.concatenate([first_grad, first_grad], axis=1)
        trails[sp] = trail[...]
        for d, c in others:
            send(trail, trails.at[sp], trail_s, trail_r, to_sp(other(d, c)))

    with jax.named_scope("pair_wait"):
        take(gw_pair, pair_r)
    gw_chip[...] = (gw_all[core].astype(F32) + gw_pair[...].astype(F32)).astype(BF16)
    for d in sorted(steps, key=abs)[::-1]:
        zz = lax.rem(z + d + nz, nz)
        send(gw_chip.at[zz], gw_in.at[z], gw_s, gw_r, to_sp(zz * 2 + core))
    pltpu.make_async_copy(gw_chip.at[z], gw_in.at[z], gw_r).start()
    take(rows.at[0, 0, pl.ds(0, rows.shape[2] // 16 * 15), :], dn_s)
    for copy in stored:
        copy.wait()
    with jax.named_scope("trail_wait"):
        take(trails.at[pl.ds(0, ns - 1)], trail_r)
    entering = jnp.zeros((1, channels), F32)
    for i in range(ns):
        entering += coef[i] * trails[i][:, :channels]
    total = grad_loc + rows_f[3] * standing(entering)
    g_rec[...] = total * rows_f[4]
    g_in[...] = total * rows_f[5]
    g_dec[...] = total * rows_f[6]
    with jax.named_scope("gw_wait"):
        take(gw_in, gw_r)
    acc = jnp.zeros(gw_in.shape[1:], F32)
    for i in range(nz):
        acc += gw_in[i].astype(F32)
    cut = g_out.shape[0]
    g_out[...] = jnp.concatenate([acc[:, :cut], acc[:, cut:]], axis=0).T

    take(trails.at[pl.ds(0, ns - 1)], trail_s)
    take(gw_pair, pair_s)
    take(gw_in.at[pl.ds(0, nz - 1)], gw_s)


def finish(count, *refs):
    held, came, left = refs[2 * count : 3 * count], refs[-2], refs[-1]
    into = [pltpu.make_async_copy(refs[n], held[n], came.at[n]) for n in range(count)]
    out = [pltpu.make_async_copy(held[n], refs[count + n], left.at[n]) for n in range(count)]
    for copy in into:
        copy.start()
    for first, second in zip(into, out):
        first.wait()
        second.start()
    for copy in out:
        copy.wait()


def shards(
    cotangent,
    normed,
    inverse_root_mean_square,
    expert_norm_scale,
    routes,
    route_probability_weight,
    gate_weight,
    up_weight,
    down_weight,
    recurrence_input,
    recurrence_gate_logits,
    input_gate_logits,
    channel_decay_weight,
    extra_log_decay,
    output_matrix,
):
    ns = lax.axis_size("sp")
    tokens, features = normed.shape
    channels = recurrence_input.shape[1]
    slots = ns * CAP
    chunks = len(CHUNKS)
    quarter = max(CHUNKS) * 2 * CAP // 4
    wide = features // SIDE
    vmem, dma = pltpu.VMEM, pltpu.SemaphoreType.DMA
    args = (
        cotangent,
        normed,
        inverse_root_mean_square.reshape(1, tokens),
        expert_norm_scale.reshape(1, features),
        routes.T,
        route_probability_weight.T,
        gate_weight,
        up_weight,
        down_weight,
        recurrence_input.T,
        recurrence_gate_logits.T,
        input_gate_logits.T,
        channel_decay_weight.reshape(1, channels),
        extra_log_decay.T,
        output_matrix.T,
    )
    f32_rows = jax.ShapeDtypeStruct((channels, tokens), F32)
    vm, hbm = pl.BlockSpec(memory_space=pltpu.VMEM), pl.BlockSpec(memory_space=pl.ANY)
    results = pl.pallas_call(
        functools.partial(kernel, ns),
        out_shape=(
            jax.ShapeDtypeStruct(gate_weight.shape, BF16),
            jax.ShapeDtypeStruct(up_weight.shape, BF16),
            jax.ShapeDtypeStruct(down_weight.shape, BF16),
            jax.ShapeDtypeStruct((features // ns, channels), F32),
            f32_rows,
            f32_rows,
            f32_rows,
        ),
        in_specs=[hbm] * len(args),
        out_specs=[hbm] * 3 + [vm] * 4,
        scratch_shapes=[
            vmem((2, slots, COLS), BF16),
            vmem((slots, tokens), BF16),
            vmem((2, SIDE, slots, wide), BF16),
            vmem((features, 2 * COLS), BF16),
            vmem((slots, 2 * COLS), BF16),
            vmem((slots, COLS), BF16),
            vmem((SIDE, SIDE, slots, COLS), BF16),
            vmem((2 * chunks, 2, SIDE, quarter, COLS), BF16),
            vmem((2 * chunks, 2, SIDE, 2 * quarter, COLS), BF16),
            vmem((2 * chunks, SIDE, 2 * quarter, COLS), BF16),
            vmem((2 * chunks, 3, 2 * quarter, COLS), BF16),
            vmem((slots, COLS), BF16),
            vmem((slots, COLS), BF16),
            vmem((SIDE, tokens, wide), BF16),
            vmem((tokens, features), BF16),
            vmem((8, channels, tokens), F32),
            vmem((tokens.bit_length() - 1, channels, tokens), F32),
            vmem((1, 2 * channels), F32),
            vmem((ns, 1, 2 * channels), F32),
            vmem((1, 2 * channels), F32),
            vmem((ns, 1, 2 * channels), F32),
            vmem((ns, 1, channels), F32),
            vmem((2, ns // 2, features // ns // 2, 2 * channels), BF16),
            vmem((ns // 2, features // ns // 2, 2 * channels), BF16),
            vmem((ns // 2, features // ns // 2, 2 * channels), BF16),
            vmem((ns // 2, features // ns // 2, 2 * channels), BF16),
            vmem((COLS, features), BF16),
            vmem((features, COLS), BF16),
            vmem((features, COLS), BF16),
            vmem((COLS, features), BF16),
            *(vmem(args[n].shape, args[n].dtype) for n in (0, 1, 2, 3, 4, 5)),
            *(vmem(a.shape, a.dtype) for a in args[9:]),
            dma((len(args),)),
            dma((3,)),
            dma,
            dma((chunks,)),
            dma,
            dma((2 * chunks, 7)),
            dma((2,)),
            dma((2 * chunks, 3)),
            dma,
            dma((2, 4)),
            dma,
            dma,
            dma,
            dma,
            dma,
            dma,
            dma,
            dma,
            dma,
            dma,
        ],
        compiler_params=pltpu.CompilerParams(
            collective_id=0, has_side_effects=True, vmem_limit_bytes=FULL
        ),
    )(*args)
    g_gate, g_up, g_down, g_out, g_rec, g_dec, g_in = pl.pallas_call(
        functools.partial(finish, len(results)),
        out_shape=tuple(jax.ShapeDtypeStruct(r.shape, r.dtype) for r in results),
        in_specs=[hbm] * len(results),
        out_specs=[hbm] * len(results),
        scratch_shapes=[vmem(r.shape, r.dtype) for r in results]
        + [dma((len(results),)), dma((len(results),))],
        compiler_params=pltpu.CompilerParams(vmem_limit_bytes=FULL),
    )(*results)
    return g_gate, g_up, g_down, g_out, g_rec.T, g_dec.T, g_in.T


def solution(mesh):
    placed = (
        P("sp", None),
        P("sp", None),
        P("sp"),
        P(),
        P("sp", None),
        P("sp", None),
        P("sp", None, "tp"),
        P("sp", None, "tp"),
        P("sp", "tp", None),
        P("sp", "tp"),
        P("sp", "tp"),
        P("sp", "tp"),
        P("tp"),
        P("sp", "tp"),
        P(None, "tp"),
    )
    return jax.shard_map(
        shards,
        mesh=mesh,
        in_specs=placed,
        out_specs=(
            P("sp", None, "tp"),
            P("sp", None, "tp"),
            P("sp", "tp", None),
            P("sp", "tp"),
            P("sp", "tp"),
            P("sp", "tp"),
            P("sp", "tp"),
        ),
        check_vma=False,
    )
```

```python
import functools

import jax
import jax.numpy as jnp
from jax import lax
from jax.experimental import pallas as pl
from jax.experimental.pallas import tpu as pltpu
from jax.sharding import PartitionSpec as P

MESH = pl.DeviceIdType.MESH
F32 = jnp.float32
BF16 = jnp.bfloat16
SIDE = 4
CHUNKS = (4, 6, 4, 2)
SOURCES = (1, -1, 2, -2, 4, -4, 5, -5, 6, -6, 7, -7, 8, 3, 0, -3)
COLS = 128
ORDER = (('begin', 0), ('near', 0), ('relay', 0, 0), ('begin', 1), ('across', 0), ('relay', 0, 2), ('relay', 0, 1), ('near', 1), ('relay', 1, 0), ('relay', 0, 3), ('begin', 2), ('across', 1), ('relay', 1, 2), ('relay', 1, 1), ('begin', 3), ('expert', 0), ('near', 2), ('relay', 2, 0), ('relay', 1, 3), ('near', 3), ('relay', 3, 0), ('mid', 0), ('across', 2), ('relay', 2, 2), ('relay', 2, 1), ('expert', 1), ('across', 3), ('relay', 3, 2), ('relay', 3, 1), ('turn', 0), ('relay', 2, 3), ('mid', 1), ('relay', 3, 3), ('expert', 2), ('give', 0), ('turn', 1), ('expert', 3), ('mid', 2), ('give', 1), ('mid', 3), ('turn', 2), ('turn', 3), ('give', 2), ('give', 3))
FIRST_EXPERT = [step for step, *_ in ORDER].index("expert")
CAP = 16
FULL = 67_043_328


def dot(a, b, ca, cb):
    return lax.dot_general(a, b, (((ca,), (cb,)), ((), ())), preferred_element_type=F32)


def take(ref, sem):
    pltpu.make_async_copy(ref, ref, sem).wait()


def send(src, dst, send_sem, recv_sem, target):
    pltpu.make_async_remote_copy(
        src_ref=src,
        dst_ref=dst,
        send_sem=send_sem,
        recv_sem=recv_sem,
        device_id=target,
        device_id_type=MESH,
    ).start()


class Flow:
    def __init__(self, piece, bulk, p, q, to_p, to_q, ss, rs):
        self.piece, self.bulk, self.p, self.q, self.to_p, self.to_q, self.ss, self.rs = (
            piece, bulk, p, q, to_p, to_q, ss, rs,
        )
        self.from_p = [p] + [lax.rem(p + SIDE - v, SIDE) for v in (1, 3, 2)]

    def along_p(self, ref, v, k):
        send(ref, ref, self.ss, self.rs.at[k], self.to_p(lax.rem(self.p + v, SIDE)))

    def along_q(self, ref, v, k):
        send(ref, ref, self.ss, self.rs.at[k], self.to_q(lax.rem(self.q + v, SIDE)))

    def mine(self, m, half=None):
        return self.piece(self.from_p[m], self.q, half)

    def other(self, m, v, half=None):
        return self.piece(self.from_p[m], lax.rem(self.q + SIDE - v, SIDE), half)

    def cross(self, m):
        self.along_q(self.mine(m), 1, 3 + m)
        self.along_q(self.mine(m), 3, 3 + m)

    def start(self):
        self.along_p(self.mine(0), 1, 0)
        self.along_p(self.mine(0), 3, 0)
        self.cross(0)

    def near(self):
        take(self.bulk(2), self.rs.at[0])
        self.along_p(self.mine(1, 0), 1, 1)
        self.along_p(self.mine(2, 1), 3, 1)
        self.cross(1)
        self.cross(2)

    def across(self):
        take(self.bulk(1), self.rs.at[1])
        self.cross(3)

    def relay(self, m):
        take(self.bulk(2), self.rs.at[3 + m])
        self.along_q(self.other(m, 1, 0), 1, 2)
        self.along_q(self.other(m, 3, 1), 3, 2)

    def last(self):
        take(self.bulk(SIDE), self.rs.at[2])


class Scatter:
    def __init__(self, block, i, axis_to, ss, rs, part, came, parts, all_came):
        self.block, self.i, self.to, self.ss, self.rs = block, i, axis_to, ss, rs
        self.part, self.came, self.parts, self.all_came = part, came, parts, all_came
        self.up, self.down, self.far = lax.rem(i + 1, 4), lax.rem(i + 3, 4), lax.rem(i + 2, 4)

    def go(self, src, dst, target, k):
        send(src, dst, self.ss, self.rs.at[k], target)

    def first(self):
        up, down = self.to(self.up), self.to(self.down)
        self.go(self.block(self.far, 0), self.part(0), up, 0)
        self.go(self.block(self.far, 1), self.part(1), down, 0)
        self.go(self.block(self.up, 1), self.came(0, 1), up, 1)
        self.go(self.block(self.down, 0), self.came(1, 0), down, 1)

    def relay(self):
        take(self.parts, self.rs.at[0])
        for member, half, dst in (
            (self.up, 0, self.came(0, 0)),
            (self.down, 1, self.came(1, 1)),
        ):
            ref = self.block(member, half)
            ref[...] = (ref[...].astype(F32) + self.part(half)[...].astype(F32)).astype(BF16)
            self.go(ref, dst, self.to(member), 1)

    def last(self):
        take(self.all_came, self.rs.at[1])

    def total(self, half):
        return (
            self.block(self.i, half)[...].astype(F32)
            + self.came(0, half)[...].astype(F32)
            + self.came(1, half)[...].astype(F32)
        )


class Direct:
    def __init__(self, block, i, axis_to, ss, rs, slot, slots):
        self.block, self.i, self.to, self.ss, self.rs = block, i, axis_to, ss, rs
        self.slot, self.slots = slot, slots

    def first(self):
        for v in (2, 1, 3):
            target = lax.rem(self.i + v, SIDE)
            send(self.block(target), self.slot(v - 1), self.ss, self.rs, self.to(target))

    def total(self):
        take(self.slots, self.rs)
        value = self.block(self.i)[...].astype(F32)
        for v in range(SIDE - 1):
            value += self.slot(v)[...].astype(F32)
        return value


def softplus(v):
    z = jnp.exp(-jnp.abs(v))
    s = z / (2.0 + z)
    q = s * s
    series = jnp.zeros_like(s)
    for k in range(9, -1, -1):
        series = series * q + 1.0 / (2 * k + 1)
    return jnp.maximum(v, 0.0) + 2.0 * s * series


def expm1(v):
    near = jnp.clip(v, -0.5, 0.5)
    series = jnp.ones_like(v)
    for k in range(10, 1, -1):
        series = 1.0 + near * series * (1.0 / k)
    return jnp.where(jnp.abs(v) < 0.5, near * series, jnp.exp(v) - 1.0)


def kernel(
    ns,
    cot_h,
    norm_h,
    irms_h,
    gain_h,
    routes_h,
    prob_h,
    gate_h,
    up_h,
    down_h,
    rec_in_h,
    rec_gate_h,
    in_gate_h,
    decay_h,
    extra_h,
    out_h,
    g_gate_h,
    g_up_h,
    g_down_h,
    g_out,
    g_rec,
    g_dec,
    g_in,
    packed,
    picked,
    rows,
    wide,
    d_wide,
    act,
    part,
    t_buf,
    c_buf,
    s_buf,
    t2_buf,
    back,
    arrived,
    dn,
    d_mix,
    rows_f,
    powers,
    lead,
    leads,
    trail,
    trails,
    coef,
    gw_all,
    gw_pair,
    gw_chip,
    gw_in,
    down_w,
    g_gate,
    g_up,
    g_down,
    cot,
    norm,
    irms,
    gain,
    routes,
    prob,
    rec_in,
    rec_gate,
    in_gate,
    decay_w,
    extra,
    out_m,
    w_r,
    g_s,
    z_s,
    z_r,
    ag_s,
    ag_r,
    rs_s,
    rs_r,
    dn_s,
    dn_r,
    back_s,
    back_r,
    lead_s,
    lead_r,
    trail_s,
    trail_r,
    pair_s,
    pair_r,
    gw_s,
    gw_r,
):
    sp, tp = lax.axis_index("sp"), lax.axis_index("tp")
    z, core = lax.div(sp, 2), lax.rem(sp, 2)
    y, x = lax.div(tp, SIDE), lax.rem(tp, SIDE)
    nz = ns // 2
    tokens = norm.shape[0]
    first_chip = [sum(CHUNKS[:k]) for k in range(len(CHUNKS) + 1)]
    row_count = [n * 2 * CAP for n in CHUNKS]
    row_base = [n * 2 * CAP for n in first_chip]
    home = SOURCES.index(0)

    def place(d):
        return SOURCES.index(d)

    def chunk_of(pos):
        return sum(pos >= first for first in first_chip[1:-1])

    def to_x(v):
        return {"sp": sp, "tp": y * SIDE + v}

    def to_y(v):
        return {"sp": sp, "tp": v * SIDE + x}

    def to_sp(v):
        return {"sp": v, "tp": tp}

    barrier = pltpu.get_barrier_semaphore()
    steps = [d for d in SOURCES if d != 0]
    others = [(d, c) for d in SOURCES for c in (0, 1) if (d, c) != (0, 0)]

    def other(d, c):
        if d == 0:
            return z * 2 + (1 - core)
        return lax.rem(z + d + nz, nz) * 2 + c

    for d, c in others:
        pl.semaphore_signal(barrier, inc=1, device_id=to_sp(other(d, c)), device_id_type=MESH)
    for v in (1, 3):
        pl.semaphore_signal(
            barrier, inc=1, device_id=to_x(lax.rem(x + v, SIDE)), device_id_type=MESH
        )
        pl.semaphore_signal(
            barrier, inc=1, device_id=to_y(lax.rem(y + v, SIDE)), device_id_type=MESH
        )

    moves = (
        (routes_h, routes),
        (prob_h, prob),
        (norm_h, norm),
        (cot_h, cot),
        (rec_gate_h, rec_gate),
        (in_gate_h, in_gate),
        (rec_in_h, rec_in),
        (decay_h, decay_w),
        (extra_h, extra),
        (gate_h.at[0], wide.at[:, :COLS]),
        (up_h.at[0], wide.at[:, COLS:]),
        (down_h.at[0], down_w),
        (irms_h, irms),
        (gain_h, gain),
        (out_h, out_m),
    )
    moves = [pltpu.make_async_copy(a, b, w_r.at[k]) for k, (a, b) in enumerate(moves)]
    for copy in moves:
        copy.start()

    def have(first, last):
        for copy in moves[first:last]:
            copy.wait()

    mine = pl.ds(pl.multiple_of(tp * COLS, COLS), COLS)
    def eye(n):
        return lax.broadcasted_iota(jnp.int32, (n, n), 0) == lax.broadcasted_iota(
            jnp.int32, (n, n), 1
        )

    square = eye(tokens)

    def upright(row):
        return jnp.sum(jnp.where(square, row, 0.0), axis=1, keepdims=True)

    have(0, 4)
    expert_id = lax.broadcasted_iota(jnp.int32, (ns, tokens), 0)
    chosen = [routes[k : k + 1, :] for k in (0, 1)]
    member = [(e == expert_id).astype(F32) for e in chosen]
    earlier = (
        lax.broadcasted_iota(jnp.int32, (tokens, tokens), 0)
        < lax.broadcasted_iota(jnp.int32, (tokens, tokens), 1)
    ).astype(BF16)
    before = dot((member[0] + member[1]).astype(BF16), earlier, 1, 0)
    slot = lax.broadcasted_iota(jnp.int32, (ns * CAP, tokens), 0).astype(F32)
    one = [
        (slot == (e.astype(F32) * CAP + jnp.sum(m * before, axis=0, keepdims=True))).astype(F32)
        for e, m in zip(chosen, member)
    ]
    both = (one[0] + one[1]).astype(BF16)
    picked[...] = both
    own_cot = cot[:, mine].astype(F32)
    packed[0] = dot(both, norm[:, mine], 1, 0).astype(BF16)
    packed[1] = (
        dot(one[0].astype(BF16), (upright(prob[0:1, :]) * own_cot).astype(BF16), 1, 0)
        + dot(one[1].astype(BF16), (upright(prob[1:2, :]) * own_cot).astype(BF16), 1, 0)
    ).astype(BF16)

    with jax.named_scope("barrier"):
        pl.semaphore_wait(barrier, len(others) + 4)

    own_x = pl.ds(pl.multiple_of(x * COLS, COLS), COLS)

    def rows_at(pos, c):
        return pl.ds(pl.multiple_of((pos * 2 + c) * CAP, CAP), CAP)

    by_chunk = [[p for p in others if chunk_of(place(p[0])) == k] for k in range(len(CHUNKS))]
    for k, (d, c) in [(k, p) for k, pairs in enumerate(by_chunk) for p in pairs[::-1]]:
        target = other(d, c)
        send(
            packed.at[:, pl.ds(pl.multiple_of(target * CAP, CAP), CAP), :],
            rows.at[:, y, rows_at(place(d), core), own_x],
            z_s,
            z_r.at[k],
            to_sp(target),
        )
    pltpu.make_async_copy(
        packed.at[:, pl.ds(pl.multiple_of(sp * CAP, CAP), CAP), :],
        rows.at[:, y, rows_at(home, core), own_x],
        z_r.at[chunk_of(home)],
    ).start()

    channels = extra.shape[0]
    corner = eye(channels)

    def lying(column):
        return jnp.sum(jnp.where(corner, column, 0.0), axis=0, keepdims=True)

    def standing(row):
        return jnp.sum(jnp.where(corner, row, 0.0), axis=1, keepdims=True)

    token = lax.broadcasted_iota(jnp.int32, (channels, tokens), 1)

    def moved(v, step, fill):
        inside = token >= step if step > 0 else token < tokens + step
        return jnp.where(inside, pltpu.roll(v, step % tokens, 1), fill)

    levels = tokens.bit_length() - 1

    def scan(a, b, sign):
        step = 1
        while step < tokens:
            b = a * moved(b, sign * step, 0.0) + b
            a = a * moved(a, sign * step, 1.0)
            step *= 2
        return a, b

    with jax.named_scope("recur"):
        have(4, 9)
        retain = jax.nn.sigmoid(rec_gate[...].astype(F32))
        admit = jax.nn.sigmoid(in_gate[...].astype(F32))
        signal = rec_in[...].astype(F32)
        speed = standing(-8.0 * softplus(-decay_w[...]))
        log_keep = retain * speed + extra[...]
        keep = jnp.exp(log_keep)
        scale_in = jnp.sqrt(-expm1(2.0 * log_keep))
        keep_cum, state_loc = scan(keep, scale_in * admit * signal, 1)
        lead[...] = jnp.concatenate(
            [lying(keep_cum[:, tokens - 1 :]), lying(state_loc[:, tokens - 1 :])], axis=1
        )
        leads[sp] = lead[...]
        for d, c in others:
            send(lead, leads.at[sp], lead_s, lead_r, to_sp(other(d, c)))
        rows_f[0] = keep_cum
        rows_f[1] = state_loc
        rows_f[2] = keep
        tail = moved(keep, -1, 1.0)
        for level in range(levels):
            powers[level] = tail
            tail = tail * moved(tail, -(1 << level), 1.0)
        rows_f[3] = tail
        rows_f[4] = scale_in * admit
        rows_f[5] = scale_in * signal * admit * (1.0 - admit)
        rows_f[6] = admit * signal * keep * keep / scale_in
        rows_f[7] = speed * retain * (1.0 - retain)

    def z_arrived(k):
        take(rows.at[:, y, pl.ds(row_base[k], row_count[k]), own_x], z_r.at[k])

    def at_x(i):
        return pl.ds(pl.multiple_of(i * COLS, COLS), COLS)

    def flows(k):
        half_rows = row_count[k] // 2

        def span(half):
            if half is None:
                return pl.ds(row_base[k], row_count[k])
            return pl.ds(row_base[k] + half * half_rows, half_rows)

        def bulk(count):
            return rows.at[0, pl.ds(0, count), span(None), pl.ds(0, COLS)]

        return (
            Flow(
                lambda p, q, h: rows.at[0, q, span(h), at_x(p)],
                bulk, x, y, to_x, to_y, ag_s, ag_r.at[2 * k],
            ),
            Flow(
                lambda p, q, h: rows.at[1, p, span(h), at_x(q)],
                bulk, y, x, to_y, to_x, ag_s, ag_r.at[2 * k + 1],
            ),
        )

    def expert(k):
        chunk = row_count[k]
        span = pl.ds(row_base[k], chunk)
        deep = rows.shape[3]
        hidden = jnp.zeros((chunk, 2 * COLS), F32)
        d_act = jnp.zeros((chunk, COLS), F32)
        for j in range(SIDE):
            hidden += dot(rows[0, j, span, :], wide[j * deep : (j + 1) * deep, :], 1, 0)
            d_act += dot(rows[1, j, span, :], down_w[:, j * deep : (j + 1) * deep], 1, 1)
        gate_pre, up_pre = hidden[:, :COLS], hidden[:, COLS:]
        sigma = jax.nn.sigmoid(gate_pre)
        swish = gate_pre * sigma
        act[span, :] = (swish * up_pre).astype(BF16)
        d_wide[span, :COLS] = (
            d_act * up_pre * sigma * (1.0 + gate_pre * (1.0 - sigma))
        ).astype(BF16)
        d_wide[span, COLS:] = (d_act * swish).astype(BF16)
        for j in range(SIDE):
            for i in range(0, SIDE, 2):
                low = (j * SIDE + i) * COLS
                piece = dot(d_wide[span, :], wide[low : low + 2 * COLS, :], 1, 1).astype(BF16)
                part[j, i, span, :] = piece[:, :COLS]
                part[j, i + 1, span, :] = piece[:, COLS:]

    def scatters(k):
        base, half, quarter = row_base[k], row_count[k] // 2, row_count[k] // 4

        def span(start, h):
            return pl.ds(start + h * quarter, quarter)

        def make(n, block, i, axis_to, i2, axis_to2):
            one = Scatter(
                block, i, axis_to, rs_s.at[0], rs_r.at[n],
                lambda h: t_buf.at[n, h, :, pl.ds(0, quarter), :],
                lambda v, h: c_buf.at[n, v, :, pl.ds(h * quarter, quarter), :],
                t_buf.at[n, :, :, pl.ds(0, quarter), :],
                c_buf.at[n, :, :, pl.ds(0, half), :],
            )
            two = Direct(
                lambda m: s_buf.at[n, m, pl.ds(0, half), :], i2, axis_to2,
                rs_s.at[1], rs_r.at[n, 2],
                lambda v: t2_buf.at[n, v, pl.ds(0, half), :],
                t2_buf.at[n, :, pl.ds(0, half), :],
            )
            return one, two

        a1, a2 = make(
            2 * k, lambda i, h: part.at[:, i, span(base, h), :], x, to_x, y, to_y
        )
        b1, b2 = make(
            2 * k + 1, lambda i, h: part.at[i, :, span(base + half, h), :], y, to_y, x, to_x
        )
        return (a1, b1), (a2, b2)

    def between(k, first):
        quarter = row_count[k] // 4
        for n, ring in enumerate(first):
            for h in (0, 1):
                s_buf[2 * k + n, :, pl.ds(h * quarter, quarter), :] = ring.total(h).astype(BF16)

    def give_back(k, second):
        half = row_count[k] // 2
        for n, ring in enumerate(second):
            back[pl.ds(row_base[k] + n * half, half), :] = ring.total().astype(BF16)
        dst = arrived.at[pl.ds(pl.multiple_of(sp * CAP, CAP), CAP), :]
        for d, c in others[::-1]:
            pos = place(-d if 0 < abs(d) < nz // 2 else d)
            if chunk_of(pos) != k:
                continue
            where = rows_at(pos, 1 - core if d == 0 else c)
            send(back.at[where, :], dst, back_s, back_r, to_sp(other(d, c)))
        if k == chunk_of(home):
            pltpu.make_async_copy(back.at[rows_at(home, core), :], dst, back_r).start()

    all_flows = [flows(k) for k in range(len(CHUNKS))]
    all_sums = [scatters(k) for k in range(len(CHUNKS))]

    def both_of(pair, name, *given):
        for one_of in pair:
            getattr(one_of, name)(*given)

    for number, (step, k, *given) in enumerate(ORDER):
        with jax.named_scope(f"{step}{k}" + "".join(f"_{m}" for m in given)):
            if step == "begin":
                z_arrived(k)
                both_of(all_flows[k], "start")
            elif step == "expert":
                if number == FIRST_EXPERT:
                    have(9, 15)
                both_of(all_flows[k], "last")
                expert(k)
                both_of(all_sums[k][0], "first")
            elif step == "mid":
                both_of(all_sums[k][0], "relay")
            elif step == "turn":
                both_of(all_sums[k][0], "last")
                between(k, all_sums[k][0])
                both_of(all_sums[k][1], "first")
            elif step == "give":
                give_back(k, all_sums[k][1])
            else:
                both_of(all_flows[k], step, *given)

    with jax.named_scope("grads"):
        deep = rows.shape[3]
        for j in range(SIDE):
            grads = dot(rows[0, j], d_wide[...], 0, 0).astype(BF16)
            g_gate[j * deep : (j + 1) * deep, :] = grads[:, :COLS]
            g_up[j * deep : (j + 1) * deep, :] = grads[:, COLS:]
            g_down[:, j * deep : (j + 1) * deep] = dot(act[...], rows[1, j], 0, 0).astype(BF16)
        stored = (
            pltpu.make_async_copy(g_gate, g_gate_h.at[0], g_s.at[0]),
            pltpu.make_async_copy(g_up, g_up_h.at[0], g_s.at[1]),
            pltpu.make_async_copy(g_down, g_down_h.at[0], g_s.at[2]),
        )
        for copy in stored:
            copy.start()

    with jax.named_scope("sent"):
        all_rows = ns * CAP
        take(packed.at[:, pl.ds(0, all_rows - CAP), :], z_s)
        take(rows.at[:, :, pl.ds(0, all_rows // 16 * 15), :], ag_s)
        take(part.at[pl.ds(0, 3)], rs_s.at[0])
        take(part.at[0, pl.ds(0, 3)], rs_s.at[1])
        take(back.at[pl.ds(0, all_rows - CAP), :], back_s)
        take(leads.at[pl.ds(0, ns - 1)], lead_s)

    with jax.named_scope("lead_wait"):
        take(leads.at[pl.ds(0, ns - 1)], lead_r)
    state_in = jnp.zeros((1, channels), F32)
    for i in range(ns):
        v = leads[i]
        state_in = jnp.where(i < sp, v[:, :channels] * state_in + v[:, channels:], state_in)
    run = jnp.ones((1, channels), F32)
    for i in range(ns):
        coef[i] = jnp.where(i > sp, run, 0.0)
        run = jnp.where(i > sp, run * leads[i][:, :channels], run)
    state_in = standing(state_in)
    state = rows_f[1] + rows_f[0] * state_in
    rows_f[6] = (moved(state, 1, state_in) * rows_f[2] - rows_f[6]) * rows_f[7]
    hidden = state.astype(BF16)

    with jax.named_scope("back_wait"):
        take(arrived, back_r)
    dn[y, :, own_x] = dot(picked[...], arrived[...], 0, 0).astype(BF16)
    half = tokens // 2

    def spot(n, i, j):
        return dn.at[j, pl.ds(n * half, half), pl.ds(pl.multiple_of(i * COLS, COLS), COLS)]

    def spread(n, i, j, along_x, slot):
        ref = spot(n, i, j)
        for v in (2, 1, 3):
            target = to_x(lax.rem(x + v, SIDE)) if along_x else to_y(lax.rem(y + v, SIDE))
            send(ref, ref, dn_s, dn_r.at[n, v - 1 if slot == 0 else 3], target)

    def back_by(p, v):
        return lax.rem(p + SIDE - v, SIDE)

    for n in (0, 1):
        spread(n, x, y, n == 0, 0)
    for n in (0, 1):
        spread(n, x, y, n == 1, 1)
    with jax.named_scope("dn_first"):
        for v in (1, 3, 2):
            for n in (0, 1):
                i, j = (back_by(x, v), y) if n == 0 else (x, back_by(y, v))
                take(spot(n, i, j), dn_r.at[n, v - 1])
                spread(n, i, j, n == 1, 1 + v)
    with jax.named_scope("dn_last"):
        for n in (0, 1):
            take(dn.at[pl.ds(0, 3), pl.ds(0, half), :], dn_r.at[n, 3])

    with jax.named_scope("mix"):
        inv_rms = upright(irms[...])
        stat = jnp.zeros((tokens, 1), F32)
        for j in range(SIDE):
            cols = pl.ds(j * deep, deep)
            g = gain[:, cols]
            stat += jnp.sum(
                (g * dn[j].astype(F32)) * (norm[:, cols].astype(F32) / g), axis=1, keepdims=True
            )
        stat = stat / norm.shape[1]
        for j in range(SIDE):
            cols = pl.ds(j * deep, deep)
            g = gain[:, cols]
            mix = cot[:, cols].astype(F32) + inv_rms * (
                g * dn[j].astype(F32) - (norm[:, cols].astype(F32) / g) * stat
            )
            d_mix[:, cols] = mix.astype(BF16)

    with jax.named_scope("gw_dot"):
        wide_piece = 2 * g_out.shape[0]
        gw = dot(hidden, d_mix[...], 1, 0)
        for n in range(nz):
            band = gw[:, n * wide_piece : (n + 1) * wide_piece]
            top, low = band[: channels // 2, :], band[channels // 2 :, :]
            cut = g_out.shape[0]
            gw_all[0, n] = jnp.concatenate([top[:, :cut], low[:, :cut]], axis=1).astype(BF16)
            gw_all[1, n] = jnp.concatenate([top[:, cut:], low[:, cut:]], axis=1).astype(BF16)

    send(gw_all.at[1 - core], gw_pair, pair_s, pair_r, to_sp(z * 2 + 1 - core))
    with jax.named_scope("trail"):
        d_state = dot(out_m[...], d_mix[...], 1, 1)
        grad_loc = d_state
        for level in range(levels):
            grad_loc += powers[level] * moved(grad_loc, -(1 << level), 0.0)
        first_grad = lying(rows_f[2][:, :1] * grad_loc[:, :1])
        trail[...] = jnp.concatenate([first_grad, first_grad], axis=1)
        trails[sp] = trail[...]
        for d, c in sorted(others, key=lambda pair: -abs(pair[0])):
            send(trail, trails.at[sp], trail_s, trail_r, to_sp(other(d, c)))

    with jax.named_scope("pair_wait"):
        take(gw_pair, pair_r)
    gw_chip[...] = (gw_all[core].astype(F32) + gw_pair[...].astype(F32)).astype(BF16)
    for d in sorted(steps, key=abs)[::-1]:
        zz = lax.rem(z + d + nz, nz)
        send(gw_chip.at[zz], gw_in.at[z], gw_s, gw_r, to_sp(zz * 2 + core))
    pltpu.make_async_copy(gw_chip.at[z], gw_in.at[z], gw_r).start()
    take(rows.at[0, 0, pl.ds(0, rows.shape[2] // 16 * 15), :], dn_s)
    for copy in stored:
        copy.wait()
    with jax.named_scope("trail_wait"):
        take(trails.at[pl.ds(0, ns - 1)], trail_r)
    entering = jnp.zeros((1, channels), F32)
    for i in range(ns):
        entering += coef[i] * trails[i][:, :channels]
    total = grad_loc + rows_f[3] * standing(entering)
    g_rec[...] = total * rows_f[4]
    g_in[...] = total * rows_f[5]
    g_dec[...] = total * rows_f[6]
    with jax.named_scope("gw_wait"):
        take(gw_in, gw_r)
    acc = jnp.zeros(gw_in.shape[1:], F32)
    for i in range(nz):
        acc += gw_in[i].astype(F32)
    cut = g_out.shape[0]
    g_out[...] = jnp.concatenate([acc[:, :cut], acc[:, cut:]], axis=0).T

    take(trails.at[pl.ds(0, ns - 1)], trail_s)
    take(gw_pair, pair_s)
    take(gw_in.at[pl.ds(0, nz - 1)], gw_s)


def finish(count, *refs):
    held, came, left = refs[2 * count : 3 * count], refs[-2], refs[-1]
    into = [pltpu.make_async_copy(refs[n], held[n], came.at[n]) for n in range(count)]
    out = [pltpu.make_async_copy(held[n], refs[count + n], left.at[n]) for n in range(count)]
    for copy in into:
        copy.start()
    for first, second in zip(into, out):
        first.wait()
        second.start()
    for copy in out:
        copy.wait()


def shards(
    cotangent,
    normed,
    inverse_root_mean_square,
    expert_norm_scale,
    routes,
    route_probability_weight,
    gate_weight,
    up_weight,
    down_weight,
    recurrence_input,
    recurrence_gate_logits,
    input_gate_logits,
    channel_decay_weight,
    extra_log_decay,
    output_matrix,
):
    ns = lax.axis_size("sp")
    tokens, features = normed.shape
    channels = recurrence_input.shape[1]
    slots = ns * CAP
    chunks = len(CHUNKS)
    quarter = max(CHUNKS) * 2 * CAP // 4
    wide = features // SIDE
    vmem, dma = pltpu.VMEM, pltpu.SemaphoreType.DMA
    args = (
        cotangent,
        normed,
        inverse_root_mean_square.reshape(1, tokens),
        expert_norm_scale.reshape(1, features),
        routes.T,
        route_probability_weight.T,
        gate_weight,
        up_weight,
        down_weight,
        recurrence_input.T,
        recurrence_gate_logits.T,
        input_gate_logits.T,
        channel_decay_weight.reshape(1, channels),
        extra_log_decay.T,
        output_matrix.T,
    )
    f32_rows = jax.ShapeDtypeStruct((channels, tokens), F32)
    vm, hbm = pl.BlockSpec(memory_space=pltpu.VMEM), pl.BlockSpec(memory_space=pl.ANY)
    results = pl.pallas_call(
        functools.partial(kernel, ns),
        out_shape=(
            jax.ShapeDtypeStruct(gate_weight.shape, BF16),
            jax.ShapeDtypeStruct(up_weight.shape, BF16),
            jax.ShapeDtypeStruct(down_weight.shape, BF16),
            jax.ShapeDtypeStruct((features // ns, channels), F32),
            f32_rows,
            f32_rows,
            f32_rows,
        ),
        in_specs=[hbm] * len(args),
        out_specs=[hbm] * 3 + [vm] * 4,
        scratch_shapes=[
            vmem((2, slots, COLS), BF16),
            vmem((slots, tokens), BF16),
            vmem((2, SIDE, slots, wide), BF16),
            vmem((features, 2 * COLS), BF16),
            vmem((slots, 2 * COLS), BF16),
            vmem((slots, COLS), BF16),
            vmem((SIDE, SIDE, slots, COLS), BF16),
            vmem((2 * chunks, 2, SIDE, quarter, COLS), BF16),
            vmem((2 * chunks, 2, SIDE, 2 * quarter, COLS), BF16),
            vmem((2 * chunks, SIDE, 2 * quarter, COLS), BF16),
            vmem((2 * chunks, 3, 2 * quarter, COLS), BF16),
            vmem((slots, COLS), BF16),
            vmem((slots, COLS), BF16),
            vmem((SIDE, tokens, wide), BF16),
            vmem((tokens, features), BF16),
            vmem((8, channels, tokens), F32),
            vmem((tokens.bit_length() - 1, channels, tokens), F32),
            vmem((1, 2 * channels), F32),
            vmem((ns, 1, 2 * channels), F32),
            vmem((1, 2 * channels), F32),
            vmem((ns, 1, 2 * channels), F32),
            vmem((ns, 1, channels), F32),
            vmem((2, ns // 2, features // ns // 2, 2 * channels), BF16),
            vmem((ns // 2, features // ns // 2, 2 * channels), BF16),
            vmem((ns // 2, features // ns // 2, 2 * channels), BF16),
            vmem((ns // 2, features // ns // 2, 2 * channels), BF16),
            vmem((COLS, features), BF16),
            vmem((features, COLS), BF16),
            vmem((features, COLS), BF16),
            vmem((COLS, features), BF16),
            *(vmem(args[n].shape, args[n].dtype) for n in (0, 1, 2, 3, 4, 5)),
            *(vmem(a.shape, a.dtype) for a in args[9:]),
            dma((len(args),)),
            dma((3,)),
            dma,
            dma((chunks,)),
            dma,
            dma((2 * chunks, 7)),
            dma((2,)),
            dma((2 * chunks, 3)),
            dma,
            dma((2, 4)),
            dma,
            dma,
            dma,
            dma,
            dma,
            dma,
            dma,
            dma,
            dma,
            dma,
        ],
        compiler_params=pltpu.CompilerParams(
            collective_id=0, has_side_effects=True, vmem_limit_bytes=FULL
        ),
    )(*args)
    g_gate, g_up, g_down, g_out, g_rec, g_dec, g_in = pl.pallas_call(
        functools.partial(finish, len(results)),
        out_shape=tuple(jax.ShapeDtypeStruct(r.shape, r.dtype) for r in results),
        in_specs=[hbm] * len(results),
        out_specs=[hbm] * len(results),
        scratch_shapes=[vmem(r.shape, r.dtype) for r in results]
        + [dma((len(results),)), dma((len(results),))],
        compiler_params=pltpu.CompilerParams(vmem_limit_bytes=FULL),
    )(*results)
    return g_gate, g_up, g_down, g_out, g_rec.T, g_dec.T, g_in.T


def solution(mesh):
    placed = (
        P("sp", None),
        P("sp", None),
        P("sp"),
        P(),
        P("sp", None),
        P("sp", None),
        P("sp", None, "tp"),
        P("sp", None, "tp"),
        P("sp", "tp", None),
        P("sp", "tp"),
        P("sp", "tp"),
        P("sp", "tp"),
        P("tp"),
        P("sp", "tp"),
        P(None, "tp"),
    )
    return jax.shard_map(
        shards,
        mesh=mesh,
        in_specs=placed,
        out_specs=(
            P("sp", None, "tp"),
            P("sp", None, "tp"),
            P("sp", "tp", None),
            P("sp", "tp"),
            P("sp", "tp"),
            P("sp", "tp"),
            P("sp", "tp"),
        ),
        check_vma=False,
    )
```
